128 devices in a mesh: fs: 16 (over z, x), tp: 8 (over y, core).
Axes of the slice: x: 4, y: 4, z: 4, core: 2. Of those that a mesh axis runs over, the one named last changes fastest.
Arguments:
- saved_input: bfloat16 [49152, 2048], P('fs'), may hold values from -6 to 6
- proj_cot: bfloat16 [3, 49152, 2048], P(None, 'fs', 'tp'), may hold values from -0.02734375 to 0.02734375
- log_cache: float32 [16, 49152], P(None, 'fs'), as said below
- cache_cot: float32 [16, 49152], P(None, 'fs'), may hold values from -0.02734375 to 0.02734375
- proj_master: float32 [3, 2048, 2048], P(None, 'fs', 'tp'), may hold values from -0.125 to 0.125
- factors: bfloat16 [3, 2048, 256], P(None, 'fs'), may hold values from -0.125 to 0.125
- first_moment: float32 [3, 256, 2048], P(None, None, 'tp'), may hold values from -6 to 6
- second_moment: float32 [3, 256, 2048], P(None, None, 'tp'), may hold values from 0.01 to 10
- gate_master: float32 [16, 2048], replicated, may hold values from -0.125 to 0.125
- gate_first: float32 [16, 2048], replicated, may hold values from -6 to 6
- gate_second: float32 [16, 2048], replicated, may hold values from 0.1 to 3
Outputs:
- proj_step: float32 [3, 2048, 2048], P(None, 'fs', 'tp')
- proj_new: float32 [3, 2048, 2048], P(None, 'fs', 'tp')
- proj_copy: bfloat16 [3, 2048, 2048], P(None, None, 'tp')
- first_new: float32 [3, 256, 2048], P(None, None, 'tp')
- second_new: float32 [3, 256, 2048], P(None, None, 'tp')
- gate_new: float32 [16, 2048], replicated
- gate_copy: bfloat16 [16, 2048], replicated
- gate_first_new: float32 [16, 2048], replicated
- gate_second_new: float32 [16, 2048], replicated
The draws below stay inside these ranges and needn't reach their ends.
Inputs may be any that keep to these rules, and one draw needn't show every extreme that they name: `log_cache`: each head's values never rise along positions.
All inputs are finite; a program needn't handle non-finite values.
Results may differ from the reference program's by a relative error of at most 0.0004.
Values may be sent and summed in bfloat16 or wider, within the bound.
A program may use at most 128 MiB of HBM per device.

```python
import math
import jax
import jax.numpy as jnp
from jax import lax

D = 2048
ATTENTION_HEADS = 16
RANK = 256
ROLES = 3
TOK_DEV = 3072
W = 2048
SEQUENCE_TOKENS = 49152


def draw_log_cache(key, part):
    keys = jax.random.split(key, 7)
    order = jax.random.permutation(keys[0], ATTENTION_HEADS)
    slow_decay = order < ATTENTION_HEADS // 2
    total = jnp.exp(jax.random.uniform(keys[1], (ATTENTION_HEADS, 1), jnp.float32, math.log(0.3), math.log(1.0)))
    fast_rate = jnp.exp(jax.random.uniform(keys[2], (ATTENTION_HEADS, 1), jnp.float32, math.log(0.01), math.log(1.0 / 30.0)))
    learning_rate = jnp.where(slow_decay[:, None], total / SEQUENCE_TOKENS, fast_rate)
    blocks = SEQUENCE_TOKENS // TOK_DEV
    block_multiplier = jnp.exp(jax.random.uniform(keys[3], (ATTENTION_HEADS, blocks), jnp.float32, math.log(0.5), math.log(2.0)))
    block_multiplier = jnp.repeat(block_multiplier, TOK_DEV, axis=1)
    coarse_estimate = jnp.exp(jax.random.uniform(keys[4], (ATTENTION_HEADS, SEQUENCE_TOKENS), jnp.float32, -0.7, 0.7))
    chosen_locations = jax.random.randint(keys[5], (ATTENTION_HEADS, 3), 0, SEQUENCE_TOKENS)
    layer_depth = jax.random.uniform(keys[6], (ATTENTION_HEADS, 3), jnp.float32, 0.22, 0.5)
    target_positions = jnp.arange(SEQUENCE_TOKENS)
    sudden_spike = jnp.zeros((ATTENTION_HEADS, SEQUENCE_TOKENS), jnp.float32)
    for position_index in range(3):
        sudden_spike = sudden_spike + jnp.where(target_positions[None, :] == chosen_locations[:, position_index:position_index + 1], layer_depth[:, position_index:position_index + 1], 0.0)
    gate_logarithm = -(learning_rate * block_multiplier * coarse_estimate) - sudden_spike * slow_decay[:, None].astype(jnp.float32)
    return jnp.cumsum(gate_logarithm, axis=1)


def draw_second_moment(key, part):
    lower, upper, fall = (1.0, 10.0, 10.0)
    base = jnp.exp(jax.random.uniform(key, (ROLES, RANK, W), jnp.float32, math.log(lower), math.log(upper)))
    column = jnp.arange(W, dtype=jnp.float32) / W
    return base * jnp.power(fall, -column)[None, None, :]


def block_levels(rng, dims, shards, smallest, largest):
    level, own = 1.0, jax.random.fold_in(rng, 6)
    for position, parts in shards:
        draws = jnp.exp(jax.random.uniform(jax.random.fold_in(own, position), (parts,), jnp.float32, smallest / len(shards), largest / len(shards)))
        level = level * jnp.repeat(draws, dims[position] // parts).reshape([-1 if axis == position else 1 for axis in range(len(dims))])
    return level


def scatter_about(stream_key, extent, spread, reach, cuts=(), held_as=jnp.bfloat16):
    factor_of = block_levels(stream_key, extent, cuts, -0.22, 0.18) if cuts else 1.0
    drawn = jax.random.normal(stream_key, extent, jnp.float32) * spread * factor_of
    return jnp.minimum(jnp.maximum(drawn, -reach), reach).astype(held_as)


def setup_inputs(seed: int = 0) -> dict:
    splits = jax.random.split(jax.random.key(seed), 12)
    saved_input = scatter_about(splits[0], (SEQUENCE_TOKENS, D), 1.0, 6.0, ((0, 16),))
    proj_cot = scatter_about(splits[1], (ROLES, SEQUENCE_TOKENS, W), SEQUENCE_TOKENS ** -0.5, 0.02734375, ((1, 16), (2, 8)))
    log_cache = draw_log_cache(jax.random.fold_in(splits[11], 71), 0)
    cache_cot = scatter_about(splits[3], (ATTENTION_HEADS, SEQUENCE_TOKENS), SEQUENCE_TOKENS ** -0.5, 0.02734375, ((1, 16),), jnp.float32)
    proj_master = scatter_about(splits[4], (ROLES, D, W), D ** -0.5, 0.125, ((1, 16), (2, 8)), jnp.float32)
    factors = scatter_about(splits[5], (ROLES, D, RANK), D ** -0.5, 0.125, ((1, 16),))
    first_moment = scatter_about(splits[6], (ROLES, RANK, W), 1.0, 6.0, ((2, 8),), jnp.float32)
    second_moment = draw_second_moment(jax.random.fold_in(splits[11], 71), 0)
    gate_master = scatter_about(splits[8], (ATTENTION_HEADS, D), D ** -0.5, 0.125, (), jnp.float32)
    gate_first = scatter_about(splits[9], (ATTENTION_HEADS, D), 1.0, 6.0, (), jnp.float32)
    gate_second = jnp.clip(jnp.exp(jax.random.uniform(splits[10], (ATTENTION_HEADS, D), jnp.float32, math.log(0.1), math.log(3.0))), 0.1, 3.0)
    return {"saved_input": saved_input, "proj_cot": proj_cot, "log_cache": log_cache, "cache_cot": cache_cot, "proj_master": proj_master, "factors": factors, "first_moment": first_moment, "second_moment": second_moment, "gate_master": gate_master, "gate_first": gate_first, "gate_second": gate_second}


BETA_ONE = 0.8
BETA_TWO = 0.9
LEARN = 0.001

def reference(saved_input, proj_cot, log_cache, cache_cot, proj_master, factors, first_moment, second_moment, gate_master, gate_first, gate_second):
    lows = []
    for role in range(ROLES):
        grad = jnp.dot(saved_input.T, proj_cot[role], preferred_element_type=jnp.float32)
        lows.append(jnp.dot(factors[role].astype(jnp.float32).T, grad, precision=lax.Precision.HIGHEST))
    low = jnp.stack(lows)
    first_new = BETA_ONE * first_moment + (1.0 - BETA_ONE) * low
    second_new = BETA_TWO * second_moment + (1.0 - BETA_TWO) * low * low
    direction = first_new / jnp.sqrt(second_new)
    scale = lax.rsqrt(jnp.mean(direction * direction) + 1e-06)
    product = jnp.einsum('rdk,rkw->rdw', factors.astype(jnp.float32), direction, precision=lax.Precision.HIGHEST)
    proj_step = scale * product
    proj_new = proj_master - LEARN * proj_step
    proj_copy = proj_new.astype(jnp.bfloat16)
    previous = jnp.concatenate([jnp.zeros((ATTENTION_HEADS, 1), jnp.float32), log_cache[:, :-1]], axis=1)
    gate_logarithm = log_cache - previous
    later = jnp.flip(jnp.cumsum(jnp.flip(cache_cot, 1), axis=1), 1)
    gate_cot = (later * -jnp.expm1(gate_logarithm)).astype(jnp.bfloat16)
    gate_grad = jnp.dot(gate_cot, saved_input, preferred_element_type=jnp.float32)
    gate_first_new = BETA_ONE * gate_first + (1.0 - BETA_ONE) * gate_grad
    gate_second_new = BETA_TWO * gate_second + (1.0 - BETA_TWO) * gate_grad * gate_grad
    gate_new = gate_master - LEARN * gate_first_new / jnp.sqrt(gate_second_new)
    gate_copy = gate_new.astype(jnp.bfloat16)
    return (proj_step, proj_new, proj_copy, first_new, second_new, gate_new, gate_copy, gate_first_new, gate_second_new)
```

```python
import functools

import jax
import jax.numpy as jnp
from jax import lax
from jax.experimental import pallas as pl
from jax.experimental.pallas import tpu as pltpu
from jax.sharding import PartitionSpec as P

BETA_ONE = 0.8
BETA_TWO = 0.9
LEARN = 0.001
MESH = pl.DeviceIdType.MESH
F32, BF16 = jnp.float32, jnp.bfloat16

FS, TP, RING = 16, 8, 4
ROLES, TOK, DIM, COLS, RANK, HEADS = 3, 3072, 2048, 256, 256, 16
BLOCK = 512
BLOCKS = DIM // BLOCK
SLICE = RANK // FS
TURN = TOK // BLOCKS


def minus_expm1(x):
    series = jnp.ones_like(x)
    for n in range(9, 1, -1):
        series = 1.0 + x * (1.0 / n) * series
    return jnp.where(jnp.abs(x) < 0.5, -x * series, 1.0 - jnp.exp(x))


def halves(x):
    upper = x.astype(BF16)
    return upper, (x - upper.astype(F32)).astype(BF16)


class Gather:
    def __init__(self, me, piece, send, recv):
        self.me, self.piece, self.send, self.recv = me, piece, send, recv
        x, z = me % RING, me // RING
        self.at = ((x, z), (z, x))

    def name(self, half, first, second):
        return second * RING + first if half == 0 else first * RING + second

    def copy(self, half, index):
        p, q = self.at[half]
        turn = lambda a, b: (a + b + RING) % RING
        if index < 3:
            d = index + 1
            out, to = (p, q), (turn(p, d), q)
            came = (turn(p, -d), q)
        else:
            e, kind = divmod(index - 3, 3)
            first = turn(p, -e)
            up = e < 2
            if kind == 0:
                out, to, came = (first, q), (p, turn(q, 1)), (first, turn(q, -1))
            elif kind == 1:
                out, to, came = (first, q), (p, turn(q, -1)), (first, turn(q, 1))
            elif up:
                out, to, came = (first, turn(q, -1)), (p, turn(q, 1)), (first, turn(q, 2))
            else:
                out, to, came = (first, turn(q, 1)), (p, turn(q, -1)), (first, turn(q, 2))
        return self.name(half, *out), self.name(half, *to), self.name(half, *came)

    def start(self, half, index):
        out, to, _ = self.copy(half, index)
        ref = self.piece(out, half)
        pltpu.make_async_remote_copy(
            ref, ref, self.send.at[half, index], self.recv.at[half, index], device_id={"fs": to}, device_id_type=MESH
        ).start()

    def waiter(self, half, index, sent):
        out, to, came = self.copy(half, index)
        ref = self.piece(out if sent else came, half)
        return pltpu.make_async_remote_copy(
            ref, ref, self.send.at[half, index], self.recv.at[half, index], device_id={"fs": to}, device_id_type=MESH
        )

    def arrived(self, half, index):
        self.waiter(half, index, False).wait_recv()

    def first(self):
        for index in (0, 1, 2, 3, 4):
            for half in (0, 1):
                self.start(half, index)

    def second(self):
        for half in (0, 1):
            self.arrived(half, 3)
            self.start(half, 5)
        for e in (1, 3, 2):
            for half in (0, 1):
                self.arrived(half, e - 1)
                self.start(half, 3 + 3 * e)
                self.start(half, 4 + 3 * e)

    def third(self):
        for e in (1, 3, 2):
            for half in (0, 1):
                self.arrived(half, 3 + 3 * e if e < 2 else 4 + 3 * e)
                self.start(half, 5 + 3 * e)

    def last(self):
        for half in (0, 1):
            for e in range(4):
                self.arrived(half, 4 + 3 * e if e < 2 else 3 + 3 * e)
                self.arrived(half, 5 + 3 * e)

    def drain(self):
        for half in (0, 1):
            for index in range(15):
                self.waiter(half, index, True).wait_send()


def kernel(
    x_hbm, cot_hbm, logs_hbm, ccot_hbm, master_hbm, factors_hbm, first_hbm, second_hbm, gm_hbm, gf_hbm, gs_hbm,
    step_ref, new_ref, copy_ref, first_ref, second_ref, gnew_ref, gcopy_ref, gfirst_ref, gsecond_ref,
    x_v, cot_v, logs_v, ccot_v, master_v, fac_v, fm_v, sm_v, gm_v, gf_v, gs_v,
    lhs_v, grad_v, later_v, gate_v, gx_v, lowp_v, rs_v, low_v, gp_v, grs_v, gfull_v, prod_v, sum_v, ss_v,
    in_sem, x_sem, cot_sem, gx_send, gx_recv, rs_send, rs_recv, ag_send, ag_recv, gr_send, gr_recv, ga_send, ga_recv,
    ss_send, ss_recv, f_send, f_recv, d_send, d_recv, c_send, c_recv,
):
    me, tp = lax.axis_index("fs"), lax.axis_index("tp")
    core = tp % 2

    def load(src, dst, sem):
        return pltpu.make_async_copy(src, dst, sem)

    fac_in = [
        load(factors_hbm.at[:, pl.ds(pl.multiple_of(64 * h + 32 * core, 32), 32), :], fac_v.at[:, 2 * me + h, core], in_sem.at[h])
        for h in (0, 1)
    ]
    logs_in = load(logs_hbm, logs_v, in_sem.at[2])
    ccot_in = load(ccot_hbm, ccot_v, in_sem.at[3])
    cot_in = [load(cot_hbm.at[r], cot_v.at[r], cot_sem.at[r]) for r in range(ROLES)]
    x_in = [load(x_hbm.at[:, pl.ds(BLOCK * n, BLOCK)], x_v.at[n], x_sem.at[n]) for n in range(BLOCKS)]
    rest_in = [
        load(s, d, in_sem.at[4 + i])
        for i, (s, d) in enumerate(
            ((first_hbm, fm_v), (second_hbm, sm_v), (master_hbm, master_v), (gm_hbm, gm_v), (gf_hbm, gf_v), (gs_hbm, gs_v))
        )
    ]
    for c in (*fac_in, ccot_in, logs_in, cot_in[0], *x_in, cot_in[1], cot_in[2], *rest_in):
        c.start()

    barrier = pltpu.get_barrier_semaphore()

    @pl.loop(1, FS)
    def _(d):
        pl.semaphore_signal(barrier, inc=1, device_id={"fs": (me + d) % FS}, device_id_type=MESH)

    @pl.loop(1, TP)
    def _(d):
        pl.semaphore_signal(barrier, inc=1, device_id={"tp": (tp + d) % TP}, device_id_type=MESH)

    ccot_in.wait()
    lane = lax.broadcasted_iota(jnp.int32, (HEADS, TOK), 1)
    later = ccot_v[...]
    by = 1
    while by < TOK:
        later = later + jnp.where(lane < TOK - by, pltpu.roll(later, TOK - by, 1), 0.0)
        by *= 2
    later_v[...] = later
    logs_in.wait()
    logs = logs_v[...]
    gate_v[...] = minus_expm1(logs - pltpu.roll(logs, 1, 1))
    small = lax.broadcasted_iota(jnp.int32, (HEADS, 128), 1)
    gx_v[me] = jnp.where(
        small < 64,
        jnp.broadcast_to(later[:, 0:1], (HEADS, 128)),
        jnp.broadcast_to(logs[:, TOK - 1 : TOK], (HEADS, 128)),
    )

    pl.semaphore_wait(barrier, FS + TP - 2)

    def to_peers(src, dst, send, recv, sem):
        @pl.loop(1, FS)
        def _(d):
            peer = (me + d) % FS
            pltpu.make_async_remote_copy(
                src(peer), dst(me), send.at[sem, d], recv.at[sem, d], device_id={"fs": peer}, device_id_type=MESH
            ).start()

    def from_peers(src, dst, send, recv, sem):
        @pl.loop(1, FS)
        def _(d):
            peer = (me - d + FS) % FS
            pltpu.make_async_remote_copy(
                src(peer), dst(peer), send.at[sem, d], recv.at[sem, d], device_id={"fs": peer}, device_id_type=MESH
            ).wait_recv()

    def sent(src, dst, send, recv, sem):
        @pl.loop(1, FS)
        def _(d):
            peer = (me + d) % FS
            pltpu.make_async_remote_copy(
                src(peer), dst(me), send.at[sem, d], recv.at[sem, d], device_id={"fs": peer}, device_id_type=MESH
            ).wait_send()

    def part(ref, r, i):
        return ref.at[r, pl.ds(pl.multiple_of(SLICE * i, SLICE), SLICE), :]

    gx = (lambda p: gx_v.at[me], lambda i: gx_v.at[i], gx_send, gx_recv, 0)
    rs = [(functools.partial(part, lowp_v, r), lambda i, r=r: rs_v.at[r, i], rs_send, rs_recv, r) for r in range(ROLES)]
    ag = [(lambda p, r=r: part(low_v, r, me), functools.partial(part, low_v, r), ag_send, ag_recv, r) for r in range(ROLES)]
    gr = (lambda p: gp_v.at[p], lambda i: grs_v.at[i], gr_send, gr_recv, 0)
    ga = (lambda p: gfull_v.at[me], lambda i: gfull_v.at[i], ga_send, ga_recv, 0)

    facs = Gather(me, lambda i, h: fac_v.at[:, 2 * i + h, core], f_send, f_recv)
    fac_in[0].wait()
    fac_in[1].wait()
    facs.first()
    to_peers(*gx)

    def across(r, side):
        return pltpu.make_async_remote_copy(
            fac_v.at[r, :, side], fac_v.at[r, :, side], d_send.at[r], d_recv.at[r],
            device_id={"tp": tp + 1 - 2 * core}, device_id_type=MESH,
        )

    def turned(r, n):
        rows = pl.ds(pl.multiple_of(TURN * n, TURN), TURN)
        lhs_v[r % 2, 0:COLS, rows] = cot_v[r, rows, :].T

    def contract(r):
        fac = fac_v[r].reshape(DIM, RANK)
        both = jnp.dot(grad_v[r], fac, preferred_element_type=F32)
        low = (both[:COLS] + both[COLS:]).T
        lowp_v[r] = low
        to_peers(*rs[r])
        rs_v[r, me] = lowp_v[r, pl.ds(pl.multiple_of(SLICE * me, SLICE), SLICE), :]

    def reduce(r):
        from_peers(*rs[r])
        low_v[r, pl.ds(pl.multiple_of(SLICE * me, SLICE), SLICE), :] = jnp.sum(rs_v[r], axis=0)
        to_peers(*ag[r])

    def finish(r):
        low = low_v[r]
        first = BETA_ONE * fm_v[r] + (1.0 - BETA_ONE) * low
        second = BETA_TWO * sm_v[r] + (1.0 - BETA_TWO) * low * low
        first_ref[r] = first
        second_ref[r] = second
        direction = first * lax.rsqrt(second)
        squares = jnp.sum((direction * direction).reshape(RANK // 8, 8, COLS), axis=0)
        squares = squares[:, :128] + squares[:, 128:]
        sum_v[...] = squares if r == 0 else sum_v[...] + squares
        own = fac_v[r, pl.ds(2 * me, 2)].reshape(128, RANK)
        both = jnp.dot(own, jnp.concatenate(halves(direction), axis=1), preferred_element_type=F32)
        prod_v[r] = both[:, :COLS] + both[:, COLS:]

    cot_in[0].wait()

    @pl.loop(0, BLOCKS)
    def _(n):
        turned(0, n)

    for r in range(ROLES):
        rows = COLS + HEADS if r == 1 else COLS
        if r + 1 < ROLES:
            cot_in[r + 1].wait()

        @pl.loop(0, BLOCKS)
        def _(n):
            if r == 0:
                load(x_hbm.at[:, pl.ds(pl.multiple_of(BLOCK * n, BLOCK), BLOCK)], x_v.at[n], x_sem.at[n]).wait()
            grad = jnp.dot(lhs_v[r % 2, 0:rows, :], x_v[n], preferred_element_type=F32)
            if r + 1 < ROLES:
                turned(r + 1, n)
            upper, lower = halves(grad[:COLS])
            span = pl.ds(pl.multiple_of(BLOCK * n, BLOCK), BLOCK)
            grad_v[r, 0:COLS, span] = upper
            grad_v[r, COLS:, span] = lower
            if r == 1:
                for i in range(BLOCK // 128):
                    gp_v[(BLOCK // 128) * n + i] = grad[COLS:, 128 * i : 128 * i + 128]
            if r == 0:
                pl.when(n == 2)(facs.second)
            if r == 1:
                pl.when(n == 1)(facs.third)
            if r == 2:
                @pl.when(n == 1)
                def _():
                    across(0, 1 - core).wait_recv()
                    contract(0)

                @pl.when(n == 2)
                def _():
                    from_peers(*gr)
                    gfull_v[me] = jnp.sum(grs_v[...], axis=0)
                    to_peers(*ga)
                    across(1, 1 - core).wait_recv()
                    contract(1)

        if r == 0:
            from_peers(*gx)
            carried = jnp.zeros((HEADS, 1), F32)
            edge = jnp.zeros((HEADS, 1), F32)
            for i in range(FS):
                message = gx_v[i]
                carried = carried + jnp.where(i > me, message[:, 0:1], 0.0)
                edge = edge + jnp.where(i == me - 1, message[:, 64:65], 0.0)
            lhs_v[1, COLS:, :] = ((later_v[...] + carried) * gate_v[...]).astype(BF16)
            start = logs_v[:, 0:128]
            start = start - jnp.where(small == 0, edge, pltpu.roll(start, 1, 1))
            lhs_v[1, COLS:, 0:128] = ((later_v[:, 0:128] + carried) * minus_expm1(start)).astype(BF16)
        if r == 1:
            to_peers(*gr)
            grs_v[me] = gp_v[me]
            facs.last()
            for k in range(ROLES):
                across(k, core).start()

    across(2, 1 - core).wait_recv()
    contract(2)
    for c in rest_in:
        c.wait()
    reduce(0)
    reduce(1)
    from_peers(*ag[0])
    finish(0)
    reduce(2)

    from_peers(*ga)
    for i in range(FS):
        cut = slice(128 * i, 128 * i + 128)
        gate = gfull_v[i]
        first = BETA_ONE * gf_v[:, cut] + (1.0 - BETA_ONE) * gate
        second = BETA_TWO * gs_v[:, cut] + (1.0 - BETA_TWO) * gate * gate
        new = gm_v[:, cut] - LEARN * (first * lax.rsqrt(second))
        gfirst_ref[:, cut] = first
        gsecond_ref[:, cut] = second
        gnew_ref[:, cut] = new
        gcopy_ref[:, cut] = new.astype(BF16)

    from_peers(*ag[1])
    finish(1)
    from_peers(*ag[2])
    finish(2)

    ss_v[tp] = sum_v[...]

    def squares_to(peer, slot, d):
        return pltpu.make_async_remote_copy(
            ss_v.at[slot], ss_v.at[slot], ss_send.at[d], ss_recv.at[d], device_id={"tp": peer}, device_id_type=MESH
        )

    @pl.loop(1, TP)
    def _(d):
        squares_to((tp + d) % TP, tp, d).start()

    @pl.loop(1, TP)
    def _(d):
        peer = (tp - d + TP) % TP
        squares_to(peer, peer, d).wait_recv()

    total = jnp.sum(jnp.sum(ss_v[...], axis=0), keepdims=True)
    scale = lax.rsqrt(total * (1.0 / (ROLES * RANK * COLS * TP)) + 1e-06)
    for r in range(ROLES):
        step = scale * prod_v[r]
        new = master_v[r] - LEARN * step
        step_ref[r] = step
        new_ref[r] = new
        copy_ref[r, pl.ds(2 * me, 2)] = new.astype(BF16).reshape(2, 64, COLS)

    copies = Gather(me, lambda i, h: copy_ref.at[:, 2 * i + h], c_send, c_recv)
    copies.first()
    copies.second()
    copies.third()
    copies.last()

    @pl.loop(1, TP)
    def _(d):
        squares_to((tp + d) % TP, tp, d).wait_send()

    for k in range(ROLES):
        across(k, core).wait_send()
        sent(*rs[k])
        sent(*ag[k])
    sent(*gx)
    sent(*gr)
    sent(*ga)
    facs.drain()
    copies.drain()


def local(*args):
    shapes = (
        ((ROLES, 128, COLS), F32),
        ((ROLES, 128, COLS), F32),
        ((ROLES, 2 * FS, 64, COLS), BF16),
        ((ROLES, RANK, COLS), F32),
        ((ROLES, RANK, COLS), F32),
        ((HEADS, DIM), F32),
        ((HEADS, DIM), BF16),
        ((HEADS, DIM), F32),
        ((HEADS, DIM), F32),
    )
    vmem, dma = pltpu.VMEM, pltpu.SemaphoreType.DMA
    gates = vmem((HEADS, DIM), F32)
    moments = vmem((ROLES, RANK, COLS), F32)
    outs = pl.pallas_call(
        kernel,
        out_shape=[jax.ShapeDtypeStruct(s, d) for s, d in shapes],
        in_specs=[pl.BlockSpec(memory_space=pl.ANY)] * 11,
        out_specs=[pl.BlockSpec(memory_space=vmem)] * 9,
        scratch_shapes=[
            vmem((BLOCKS, TOK, BLOCK), BF16),
            vmem((ROLES, TOK, COLS), BF16),
            vmem((HEADS, TOK), F32),
            vmem((HEADS, TOK), F32),
            vmem((ROLES, 128, COLS), F32),
            vmem((ROLES, 2 * FS, 2, 32, RANK), BF16),
            moments, moments, gates, gates, gates,
            vmem((2, COLS + HEADS, TOK), BF16),
            vmem((ROLES, 2 * COLS, DIM), BF16),
            vmem((HEADS, TOK), F32),
            vmem((HEADS, TOK), F32),
            vmem((FS, HEADS, 128), F32),
            moments,
            vmem((ROLES, FS, SLICE, COLS), F32),
            moments,
            vmem((FS, HEADS, 128), F32),
            vmem((FS, HEADS, 128), F32),
            vmem((FS, HEADS, 128), F32),
            vmem((ROLES, 128, COLS), F32),
            vmem((8, 128), F32),
            vmem((TP, 8, 128), F32),
            dma((10,)), dma((BLOCKS,)), dma((ROLES,)),
            dma((1, FS)), dma((1, FS)),
            dma((ROLES, FS)), dma((ROLES, FS)), dma((ROLES, FS)), dma((ROLES, FS)),
            dma((1, FS)), dma((1, FS)), dma((1, FS)), dma((1, FS)),
            dma((TP,)), dma((TP,)),
            dma((2, 15)), dma((2, 15)), dma((ROLES,)), dma((ROLES,)), dma((2, 15)), dma((2, 15)),
        ],
        compiler_params=pltpu.CompilerParams(
            collective_id=0, has_side_effects=True, vmem_limit_bytes=56 * 1024 * 1024
        ),
    )(*args)
    outs = list(outs)
    outs[2] = outs[2].reshape(ROLES, DIM, COLS)
    return tuple(outs)


def solution(mesh):
    placed = (
        P("fs", None),
        P(None, "fs", "tp"),
        P(None, "fs"),
        P(None, "fs"),
        P(None, "fs", "tp"),
        P(None, "fs", None),
        P(None, None, "tp"),
        P(None, None, "tp"),
        P(),
        P(),
        P(),
    )
    return jax.shard_map(
        local,
        mesh=mesh,
        in_specs=placed,
        out_specs=(
            P(None, "fs", "tp"),
            P(None, "fs", "tp"),
            P(None, None, "tp"),
            P(None, None, "tp"),
            P(None, None, "tp"),
            P(),
            P(),
            P(),
            P(),
        ),
        check_vma=False,
    )
```

```python
import functools

import jax
import jax.numpy as jnp
from jax import lax
from jax.experimental import pallas as pl
from jax.experimental.pallas import tpu as pltpu
from jax.sharding import PartitionSpec as P

BETA_ONE = 0.8
BETA_TWO = 0.9
LEARN = 0.001
MESH = pl.DeviceIdType.MESH
F32, BF16 = jnp.float32, jnp.bfloat16

FS, TP, RING = 16, 8, 4
ROLES, TOK, DIM, COLS, RANK, HEADS = 3, 3072, 2048, 256, 256, 16
BLOCK = 512
BLOCKS = DIM // BLOCK
TURN = TOK // BLOCKS


def minus_expm1(x):
    series = jnp.ones_like(x)
    for n in range(9, 1, -1):
        series = 1.0 + x * (1.0 / n) * series
    return jnp.where(jnp.abs(x) < 0.5, -x * series, 1.0 - jnp.exp(x))


def halves(x):
    upper = x.astype(BF16)
    return upper, (x - upper.astype(F32)).astype(BF16)


class Gather:
    def __init__(self, me, piece, many, send, recv):
        self.me, self.piece, self.many, self.send, self.recv = me, piece, many, send, recv
        x, z = me % RING, me // RING
        self.at = ((x, z), (z, x))

    def name(self, half, first, second):
        return second * RING + first if half == 0 else first * RING + second

    def sem(self, half, index):
        if index < 3:
            return self.recv.at[7 * half + index]
        e, kind = divmod(index - 3, 3)
        if kind == (0 if e == 0 else 1):
            return self.recv.at[7 * half + 3 + e]
        return self.recv.at[14]

    def copy(self, half, index):
        p, q = self.at[half]
        turn = lambda a, b: (a + b + RING) % RING
        if index < 3:
            d = index + 1
            out, to, came = (p, q), (turn(p, d), q), (turn(p, -d), q)
        else:
            e, kind = divmod(index - 3, 3)
            first = turn(p, -e)
            if kind == 0:
                out, to, came = (first, q), (p, turn(q, 1)), (first, turn(q, -1))
            elif kind == 1:
                out, to, came = (first, q), (p, turn(q, -1)), (first, turn(q, 1))
            elif e == 0:
                out, to, came = (first, turn(q, -1)), (p, turn(q, 1)), (first, turn(q, 2))
            else:
                out, to, came = (first, turn(q, 1)), (p, turn(q, -1)), (first, turn(q, 2))
        ref = self.piece(self.name(half, *out), half)
        got = self.piece(self.name(half, *came), half)
        to = {"fs": self.name(half, *to)}
        make = lambda r: pltpu.make_async_remote_copy(
            r, r, self.send, self.sem(half, index), device_id=to, device_id_type=MESH
        )
        return make(ref), make(got)

    def start(self, half, index):
        self.copy(half, index)[0].start()

    def arrived(self, half, index):
        self.copy(half, index)[1].wait_recv()

    def first(self):
        for index in (1, 0, 2, 3, 4):
            for half in (0, 1):
                self.start(half, index)

    def second(self):
        for half in (0, 1):
            self.arrived(half, 3)
            self.start(half, 5)
        for e in (1, 3, 2):
            for half in (0, 1):
                self.arrived(half, e - 1)
                self.start(half, 3 + 3 * e)
                self.start(half, 4 + 3 * e)

    def third(self):
        for e in (1, 3, 2):
            for half in (0, 1):
                self.arrived(half, 4 + 3 * e)
                self.start(half, 5 + 3 * e)

    def whole(self, n, sem):
        ref = self.many(n)
        return pltpu.make_async_remote_copy(
            ref, ref, self.send, sem, device_id={"fs": (self.me + 1) % FS}, device_id_type=MESH
        )

    def last(self):
        self.whole(16, self.recv.at[14]).wait_recv()

    def drain(self):
        self.whole(30, self.recv.at[14]).wait_send()


def kernel(
    x_hbm, cot_hbm, logs_hbm, ccot_hbm, master_hbm, factors_hbm, first_hbm, second_hbm, gm_hbm, gf_hbm, gs_hbm,
    step_ref, new_ref, copy_ref, first_ref, second_ref, gnew_ref, gcopy_ref, gfirst_ref, gsecond_ref,
    x_v, cot_v, logs_v, ccot_v, master_v, fac_v, fm_v, sm_v, gm_v, gf_v, gs_v,
    lhs_v, grad_v, later_v, gate_v, gx_v, lowp_v, sum_a, sum_b, sum_c, low_v, gp_v, grs_v, gfull_v, prod_v, ss_v, st_v,
    in_sem, x_sem, cot_sem, p_send, p_recv, s_send, s_recv, ss_sem, f_send, f_recv, d_send, d_recv, c_send, c_recv,
):
    me, tp = lax.axis_index("fs"), lax.axis_index("tp")
    core = tp % 2

    def load(src, dst, sem):
        return pltpu.make_async_copy(src, dst, sem)

    fac_in = [
        load(factors_hbm.at[:, pl.ds(pl.multiple_of(64 * h + 32 * core, 32), 32), :], fac_v.at[:, 2 * me + h, core], in_sem.at[h])
        for h in (0, 1)
    ]
    logs_in = load(logs_hbm, logs_v, in_sem.at[2])
    ccot_in = load(ccot_hbm, ccot_v, in_sem.at[3])
    cot_in = [load(cot_hbm.at[r], cot_v.at[r], cot_sem.at[r]) for r in range(ROLES)]
    x_in = [load(x_hbm.at[:, pl.ds(BLOCK * n, BLOCK)], x_v.at[n], x_sem.at[n]) for n in range(BLOCKS)]
    rest_in = [
        load(s, d, in_sem.at[4 + i])
        for i, (s, d) in enumerate(
            ((first_hbm, fm_v), (second_hbm, sm_v), (master_hbm, master_v), (gm_hbm, gm_v), (gf_hbm, gf_v), (gs_hbm, gs_v))
        )
    ]
    for c in (*fac_in, ccot_in, logs_in, cot_in[0], x_in[0], cot_in[1], *x_in[1:], cot_in[2], *rest_in):
        c.start()

    barrier = pltpu.get_barrier_semaphore()

    @pl.loop(1, FS)
    def _(d):
        pl.semaphore_signal(barrier, inc=1, device_id={"fs": (me + d) % FS}, device_id_type=MESH)

    @pl.loop(1, TP)
    def _(d):
        pl.semaphore_signal(barrier, inc=1, device_id={"tp": (tp + d) % TP}, device_id_type=MESH)

    def put(src, dst, send, recv, to):
        return pltpu.make_async_remote_copy(src, dst, send, recv, device_id=to, device_id_type=MESH)

    def to_peers(src, dst, k):
        @pl.loop(1, FS)
        def _(d):
            peer = (me + d) % FS
            put(src(peer), dst, p_send.at[k], p_recv.at[k], {"fs": peer}).start()

    def from_peers(ref, k):
        ref = ref.at[pl.ds(0, FS - 1)]
        put(ref, ref, p_send.at[k], p_recv.at[k], {"fs": (me + 1) % FS}).wait_recv()

    def sent(ref, k):
        ref = ref.at[pl.ds(0, FS - 1)]
        put(ref, ref, p_send.at[k], p_recv.at[k], {"fs": (me + 1) % FS}).wait_send()

    me_x, me_z = me % RING, me // RING
    at = ((me_x, me_z), (me_z, me_x))

    def device(half, first, second):
        return {"fs": second * RING + first if half == 0 else first * RING + second}

    def turn(a, d):
        return (a + d) % RING

    def rows(start, size):
        return pl.ds(pl.multiple_of(start, 8), size)

    def swap(r, phase):
        for half in (0, 1):
            p, q = at[half]
            for d in (1, 3, 2):
                if phase == 0:
                    to = (turn(p, d), q)
                    src = lowp_v.at[r, rows(128 * half + 32 * to[0], 32)]
                    dst = sum_a.at[r, half, d - 1]
                elif phase == 1:
                    to = (p, turn(q, d))
                    src = sum_b.at[r, half, rows(8 * to[1], 8)]
                    dst = sum_c.at[r, half, d - 1]
                elif phase == 2:
                    to = (p, turn(q, d))
                    src = dst = low_v.at[r, rows(128 * half + 32 * p + 8 * q, 8)]
                else:
                    to = (turn(p, d), q)
                    src = dst = low_v.at[r, rows(128 * half + 32 * p, 32)]
                put(src, dst, s_send.at[r, phase], s_recv.at[r, phase], device(half, *to)).start()

    def whole(r, phase):
        ref = (sum_a.at[r], sum_c.at[r], low_v.at[r, pl.ds(0, 48)], low_v.at[r, pl.ds(0, 192)])[phase]
        return put(ref, ref, s_send.at[r, phase], s_recv.at[r, phase], {"fs": (me + 1) % FS})

    def second_sum(r):
        whole(r, 0).wait_recv()
        for half in (0, 1):
            p, q = at[half]
            got = sum_a[r, half]
            sum_b[r, half] = lowp_v[r, rows(128 * half + 32 * p, 32)] + got[0] + got[1] + got[2]
        swap(r, 1)

    def first_spread(r):
        whole(r, 1).wait_recv()
        for half in (0, 1):
            p, q = at[half]
            got = sum_c[r, half]
            low_v[r, rows(128 * half + 32 * p + 8 * q, 8)] = sum_b[r, half, rows(8 * q, 8)] + got[0] + got[1] + got[2]
        swap(r, 2)

    def second_spread(r):
        whole(r, 2).wait_recv()
        swap(r, 3)

    ccot_in.wait()
    logs_in.wait()
    small = lax.broadcasted_iota(jnp.int32, (8, 128), 1)
    sums = jnp.sum(ccot_v[...], axis=1, keepdims=True)
    ends = logs_v[:, TOK - 128 :][:, 127:128]
    message = jnp.where(small < 32, sums[:8], sums[8:])
    message = jnp.where(small < 64, message, ends[:8])
    gx_v[me] = jnp.where(small < 96, message, ends[8:])

    facs = [
        Gather(
            me,
            lambda i, h, r=r: fac_v.at[r, 2 * i + h, core],
            lambda n, r=r: fac_v.at[r, pl.ds(0, n), core],
            f_send.at[r],
            f_recv.at[r],
        )
        for r in range(ROLES)
    ]
    fac_in[0].wait()
    fac_in[1].wait()
    pl.semaphore_wait(barrier, FS + TP - 2)
    to_peers(lambda peer: gx_v.at[me], gx_v.at[me], 0)
    for r in range(ROLES):
        facs[r].first()

    lane = lax.broadcasted_iota(jnp.int32, (HEADS, TOK), 1)
    later = ccot_v[...]
    by = 1
    while by < TOK:
        later = later + jnp.where(lane < TOK - by, pltpu.roll(later, TOK - by, 1), 0.0)
        by *= 2
    later_v[...] = later
    logs = logs_v[...]
    gate_v[...] = minus_expm1(logs - pltpu.roll(logs, 1, 1))

    def across(r, side):
        return pltpu.make_async_remote_copy(
            fac_v.at[r, :, side], fac_v.at[r, :, side], d_send.at[r], d_recv.at[r],
            device_id={"tp": tp + 1 - 2 * core}, device_id_type=MESH,
        )

    def turned(r, n):
        span = pl.ds(pl.multiple_of(TURN * n, TURN), TURN)
        lhs_v[r % 2, 0:COLS, span] = cot_v[r, span, :].T

    def contract(r):
        fac = fac_v[r].reshape(DIM, RANK)
        both = jnp.dot(grad_v[r], fac, preferred_element_type=F32)
        lowp_v[r] = (both[:COLS] + both[COLS:]).T
        swap(r, 0)

    def finish(r):
        low = low_v[r]
        first = BETA_ONE * fm_v[r] + (1.0 - BETA_ONE) * low
        second = BETA_TWO * sm_v[r] + (1.0 - BETA_TWO) * low * low
        first_ref[r] = first
        second_ref[r] = second
        direction = first * lax.rsqrt(second)
        own = fac_v[r, pl.ds(2 * me, 2)].reshape(128, RANK)
        both = jnp.dot(own, jnp.concatenate(halves(direction), axis=1), preferred_element_type=F32)
        prod_v[r] = both[:, :COLS] + both[:, COLS:]

    cot_in[0].wait()

    @pl.loop(0, BLOCKS)
    def _(n):
        turned(0, n)

    def handed(r):
        facs[r].last()
        across(r, core).start()

    def joined(r):
        across(r, 1 - core).wait_recv()
        contract(r)

    events = (
        ((1, facs[0].second), (2, facs[1].second), (3, facs[2].second)),
        (
            (0, facs[0].third),
            (1, facs[1].third),
            (2, facs[2].third),
            (2, functools.partial(handed, 0)),
            (3, functools.partial(handed, 1)),
        ),
        ((0, functools.partial(handed, 2)), (1, functools.partial(joined, 0)), (2, functools.partial(joined, 1))),
    )

    for r in range(ROLES):
        height = COLS + HEADS if r == 1 else COLS

        @pl.loop(0, BLOCKS)
        def _(n):
            if r == 0:
                load(x_hbm.at[:, pl.ds(pl.multiple_of(BLOCK * n, BLOCK), BLOCK)], x_v.at[n], x_sem.at[n]).wait()
            grad = jnp.dot(lhs_v[r % 2, 0:height, :], x_v[n], preferred_element_type=F32)
            if r + 1 < ROLES:
                pl.when(n == 0)(cot_in[r + 1].wait)
                turned(r + 1, n)
            upper, lower = halves(grad[:COLS])
            span = pl.ds(pl.multiple_of(BLOCK * n, BLOCK), BLOCK)
            grad_v[r, 0:COLS, span] = upper
            grad_v[r, COLS:, span] = lower
            if r == 1:
                for i in range(BLOCK // 128):
                    gp_v[(BLOCK // 128) * n + i] = grad[COLS:, 128 * i : 128 * i + 128]
            for event, work in events[r]:
                pl.when(n == event)(work)

        if r == 0:
            from_peers(gx_v, 0)
            carried = jnp.zeros((8, 128), F32)
            edge = jnp.zeros((8, 128), F32)
            for i in range(FS):
                message = gx_v[i]
                carried = carried + jnp.where(i > me, message, 0.0)
                edge = edge + jnp.where(i == me - 1, message, 0.0)
            carried = jnp.concatenate([carried[:, 0:1], carried[:, 32:33]], axis=0)
            edge = jnp.concatenate([edge[:, 64:65], edge[:, 96:97]], axis=0)
            lhs_v[1, COLS:, :] = ((later_v[...] + carried) * gate_v[...]).astype(BF16)
            start = logs_v[:, 0:128]
            start = start - jnp.where(lane[:, 0:128] == 0, edge, pltpu.roll(start, 1, 1))
            lhs_v[1, COLS:, 0:128] = ((later_v[:, 0:128] + carried) * minus_expm1(start)).astype(BF16)
        if r == 1:
            to_peers(lambda peer: gp_v.at[peer], grs_v.at[me], 1)
            grs_v[me] = gp_v[me]

    joined(2)
    for c in rest_in:
        c.wait()

    def slice_squares(r):
        squares = jnp.zeros((8, COLS), F32)
        for half in (0, 1):
            p, q = at[half]
            own = rows(128 * half + 32 * p + 8 * q, 8)
            low = low_v[r, own]
            first = BETA_ONE * fm_v[r, own] + (1.0 - BETA_ONE) * low
            second = BETA_TWO * sm_v[r, own] + (1.0 - BETA_TWO) * low * low
            direction = first * lax.rsqrt(second)
            squares = squares + direction * direction
        return squares[:, :128] + squares[:, 128:]

    from_peers(grs_v, 1)
    gfull_v[me] = jnp.sum(grs_v[...], axis=0)
    second_sum(0)
    second_sum(1)
    first_spread(0)
    second_sum(2)
    first_spread(1)
    second_spread(0)
    first_spread(2)

    ss_v[tp] = slice_squares(0) + slice_squares(1) + slice_squares(2)

    @pl.loop(1, TP)
    def _(d):
        put(ss_v.at[tp], ss_v.at[tp], ss_sem.at[0], ss_sem.at[1], {"tp": (tp + d) % TP}).start()

    squares = put(ss_v.at[pl.ds(0, TP - 1)], ss_v.at[pl.ds(0, TP - 1)], ss_sem.at[0], ss_sem.at[1], {"tp": (tp + 1) % TP})
    to_peers(lambda peer: gfull_v.at[me], gfull_v.at[me], 2)
    second_spread(1)
    squares.wait_recv()
    st_v[me] = jnp.sum(ss_v[...], axis=0)
    to_peers(lambda peer: st_v.at[me], st_v.at[me], 3)
    second_spread(2)
    whole(0, 3).wait_recv()
    finish(0)
    whole(1, 3).wait_recv()
    finish(1)
    whole(2, 3).wait_recv()
    finish(2)

    from_peers(st_v, 3)
    total = jnp.sum(jnp.sum(st_v[...], axis=0), keepdims=True)
    scale = lax.rsqrt(total * (1.0 / (ROLES * RANK * COLS * TP)) + 1e-06)
    copies = [
        Gather(
            me, lambda i, h, r=r: copy_ref.at[r, 2 * i + h], lambda n, r=r: copy_ref.at[r, pl.ds(0, n)], c_send.at[r], c_recv.at[r]
        )
        for r in range(ROLES)
    ]
    for r in range(ROLES):
        step = scale * prod_v[r]
        new = master_v[r] - LEARN * step
        step_ref[r] = step
        new_ref[r] = new
        copy_ref[r, pl.ds(2 * me, 2)] = new.astype(BF16).reshape(2, 64, COLS)
        copies[r].first()

    from_peers(gfull_v, 2)
    for i in range(FS):
        cut = slice(128 * i, 128 * i + 128)
        gate = gfull_v[i]
        first = BETA_ONE * gf_v[:, cut] + (1.0 - BETA_ONE) * gate
        second = BETA_TWO * gs_v[:, cut] + (1.0 - BETA_TWO) * gate * gate
        new = gm_v[:, cut] - LEARN * (first * lax.rsqrt(second))
        gfirst_ref[:, cut] = first
        gsecond_ref[:, cut] = second
        gnew_ref[:, cut] = new
        gcopy_ref[:, cut] = new.astype(BF16)
    squares.wait_send()
    for r in range(ROLES):
        across(r, core).wait_send()
        for phase in range(4):
            whole(r, phase).wait_send()
    sent(gx_v, 0)
    sent(gp_v, 1)
    sent(gfull_v, 2)
    sent(st_v, 3)
    for r in range(ROLES):
        facs[r].drain()

    for step in ("second", "third", "last", "drain"):
        for gather in copies:
            getattr(gather, step)()


def written(*refs):
    copies = [pltpu.make_async_copy(refs[i], refs[9 + i], refs[18].at[i]) for i in range(9)]
    for c in copies:
        c.start()
    for c in copies:
        c.wait()


def local(*args):
    shapes = (
        ((ROLES, 128, COLS), F32),
        ((ROLES, 128, COLS), F32),
        ((ROLES, 2 * FS, 64, COLS), BF16),
        ((ROLES, RANK, COLS), F32),
        ((ROLES, RANK, COLS), F32),
        ((HEADS, DIM), F32),
        ((HEADS, DIM), BF16),
        ((HEADS, DIM), F32),
        ((HEADS, DIM), F32),
    )
    vmem, dma = pltpu.VMEM, pltpu.SemaphoreType.DMA
    gates = vmem((HEADS, DIM), F32)
    moments = vmem((ROLES, RANK, COLS), F32)
    outs = pl.pallas_call(
        kernel,
        out_shape=[vmem(s, d) for s, d in shapes],
        in_specs=[pl.BlockSpec(memory_space=pl.ANY)] * 11,
        out_specs=[pl.BlockSpec(memory_space=vmem)] * 9,
        scratch_shapes=[
            vmem((BLOCKS, TOK, BLOCK), BF16),
            vmem((ROLES, TOK, COLS), BF16),
            vmem((HEADS, TOK), F32),
            vmem((HEADS, TOK), F32),
            vmem((ROLES, 128, COLS), F32),
            vmem((ROLES, 2 * FS, 2, 32, RANK), BF16),
            moments, moments, gates, gates, gates,
            vmem((2, COLS + HEADS, TOK), BF16),
            vmem((ROLES, 2 * COLS, DIM), BF16),
            vmem((HEADS, TOK), F32),
            vmem((HEADS, TOK), F32),
            vmem((FS, 8, 128), F32),
            moments,
            vmem((ROLES, 2, 3, 32, COLS), F32),
            vmem((ROLES, 2, 32, COLS), F32),
            vmem((ROLES, 2, 3, 8, COLS), F32),
            moments,
            vmem((FS, HEADS, 128), F32),
            vmem((FS, HEADS, 128), F32),
            vmem((FS, HEADS, 128), F32),
            vmem((ROLES, 128, COLS), F32),
            vmem((TP, 8, 128), F32),
            vmem((FS, 8, 128), F32),
            dma((10,)), dma((BLOCKS,)), dma((ROLES,)),
            dma((4,)), dma((4,)), dma((ROLES, 4)), dma((ROLES, 4)), dma((2,)),
            dma((ROLES,)), dma((ROLES, 15)), dma((ROLES,)), dma((ROLES,)), dma((ROLES,)), dma((ROLES, 15)),
        ],
        compiler_params=pltpu.CompilerParams(
            collective_id=0, has_side_effects=True, vmem_limit_bytes=57 * 1024 * 1024
        ),
    )(*args)
    outs = pl.pallas_call(
        written,
        out_shape=[jax.ShapeDtypeStruct(s, d) for s, d in shapes],
        in_specs=[pl.BlockSpec(memory_space=vmem)] * 9,
        out_specs=[pl.BlockSpec(memory_space=pl.ANY)] * 9,
        scratch_shapes=[dma((9,))],
        compiler_params=pltpu.CompilerParams(vmem_limit_bytes=1024 * 1024),
    )(*(pltpu.with_memory_space_constraint(o, pltpu.VMEM) for o in outs))
    outs = list(outs)
    outs[2] = outs[2].reshape(ROLES, DIM, COLS)
    return tuple(outs)


def solution(mesh):
    placed = (
        P("fs", None),
        P(None, "fs", "tp"),
        P(None, "fs"),
        P(None, "fs"),
        P(None, "fs", "tp"),
        P(None, "fs", None),
        P(None, None, "tp"),
        P(None, None, "tp"),
        P(),
        P(),
        P(),
    )
    return jax.shard_map(
        local,
        mesh=mesh,
        in_specs=placed,
        out_specs=(
            P(None, "fs", "tp"),
            P(None, "fs", "tp"),
            P(None, None, "tp"),
            P(None, None, "tp"),
            P(None, None, "tp"),
            P(),
            P(),
            P(),
            P(),
        ),
        check_vma=False,
    )
```

```python
import functools

import jax
import jax.numpy as jnp
from jax import lax
from jax.experimental import pallas as pl
from jax.experimental.pallas import tpu as pltpu
from jax.sharding import PartitionSpec as P

BETA_ONE = 0.8
BETA_TWO = 0.9
LEARN = 0.001
MESH = pl.DeviceIdType.MESH
F32, BF16 = jnp.float32, jnp.bfloat16

FS, TP, RING = 16, 8, 4
ROLES, TOK, DIM, COLS, RANK, HEADS = 3, 3072, 2048, 256, 256, 16
BLOCK = 512
BLOCKS = DIM // BLOCK
EARLY = 16
TURN = TOK // BLOCKS


def minus_expm1(x):
    series = jnp.ones_like(x)
    for n in range(9, 1, -1):
        series = 1.0 + x * (1.0 / n) * series
    return jnp.where(jnp.abs(x) < 0.5, -x * series, 1.0 - jnp.exp(x))


def halves(x):
    upper = x.astype(BF16)
    return upper, (x - upper.astype(F32)).astype(BF16)


class Gather:
    def __init__(self, me, piece, many, send, recv, coarse=False):
        self.me, self.piece, self.many, self.send, self.recv, self.coarse = me, piece, many, send, recv, coarse
        x, z = me % RING, me // RING
        self.at = ((x, z), (z, x))

    def name(self, half, first, second):
        return second * RING + first if half == 0 else first * RING + second

    def sem(self, index):
        if index < 3:
            return self.recv.at[1 if self.coarse else 1 + index]
        e, kind = divmod(index - 3, 3)
        if kind == (0 if e < 2 else 1):
            return self.recv.at[(1 if e == 0 else 2) if self.coarse else 4 + e]
        return self.recv.at[0]

    def copy(self, half, index):
        p, q = self.at[half]
        turn = lambda a, b: (a + b + RING) % RING
        if index < 3:
            d = index + 1
            out, to = (p, q), (turn(p, d), q)
        else:
            e, kind = divmod(index - 3, 3)
            first = turn(p, -e)
            if kind == 0:
                out, to = (first, q), (p, turn(q, 1))
            elif kind == 1:
                out, to = (first, q), (p, turn(q, -1))
            elif e < 2:
                out, to = (first, turn(q, -1)), (p, turn(q, 1))
            else:
                out, to = (first, turn(q, 1)), (p, turn(q, -1))
        ref = self.piece(self.name(half, *out), half)
        return pltpu.make_async_remote_copy(
            ref, ref, self.send, self.sem(index), device_id={"fs": self.name(half, *to)}, device_id_type=MESH
        )

    def start(self, index):
        for half in (0, 1):
            self.copy(half, index).start()

    def arrived(self, index):
        self.whole(2, self.sem(index)).wait_recv()

    def first(self):
        for index in (1, 0, 2, 3, 4):
            self.start(index)

    def second(self, own=True, behind=(1, 3, 2)):
        if self.coarse:
            self.whole(8, self.recv.at[1]).wait_recv()
        if own:
            if not self.coarse:
                self.arrived(3)
            self.start(5)
        for e in behind:
            if not self.coarse:
                self.arrived(e - 1)
            self.start(3 + 3 * e)
            self.start(4 + 3 * e)

    def third(self):
        if self.coarse:
            self.whole(6, self.recv.at[2]).wait_recv()
        for e in (1, 3, 2):
            if not self.coarse:
                self.arrived(3 + 3 * e if e < 2 else 4 + 3 * e)
            self.start(5 + 3 * e)

    def whole(self, n, sem):
        ref = self.many(n)
        return pltpu.make_async_remote_copy(
            ref, ref, self.send, sem, device_id={"fs": (self.me + 1) % FS}, device_id_type=MESH
        )

    def last(self):
        self.whole(16, self.recv.at[0]).wait_recv()

    def drain(self):
        self.whole(30, self.recv.at[0]).wait_send()


def kernel(
    x_hbm, cot_hbm, logs_hbm, ccot_hbm, master_hbm, factors_hbm, first_hbm, second_hbm, gm_hbm, gf_hbm, gs_hbm,
    step_ref, new_ref, copy_ref, first_ref, second_ref, gnew_ref, gcopy_ref, gfirst_ref, gsecond_ref,
    x_v, cot_v, logs_v, ccot_v, master_v, fac_v, fm_v, sm_v, gm_v, gf_v, gs_v,
    lhs_v, grad_v, later_v, gate_v, gx_v, lowp_v, sum_a, sum_b, sum_c, low_v, gp_v, grs_v, gfull_v, prod_v, ss_v, st_v, early_v, dir_v,
    in_sem, x_sem, cot_sem, p_send, p_recv, s_send, s_recv, ss_sem, f_send, f_recv, d_send, d_recv, c_send, c_recv, e_send, e_recv,
):
    me, tp = lax.axis_index("fs"), lax.axis_index("tp")
    core = tp % 2

    def load(src, dst, sem):
        return pltpu.make_async_copy(src, dst, sem)

    fac_in = [
        load(factors_hbm.at[:, pl.ds(pl.multiple_of(64 * h + 32 * core, 32), 32), :], fac_v.at[:, 2 * me + h, core], in_sem.at[h])
        for h in (0, 1)
    ]
    logs_in = load(logs_hbm, logs_v, in_sem.at[2])
    ccot_in = load(ccot_hbm, ccot_v, in_sem.at[3])
    cot_in = [load(cot_hbm.at[r], cot_v.at[r], cot_sem.at[r]) for r in range(ROLES)]
    x_in = [load(x_hbm.at[:, pl.ds(BLOCK * n, BLOCK)], x_v.at[n], x_sem.at[n]) for n in range(BLOCKS)]
    rest_in = [
        load(s, d, in_sem.at[4 + i])
        for i, (s, d) in enumerate(
            ((first_hbm, fm_v), (second_hbm, sm_v), (master_hbm, master_v), (gm_hbm, gm_v), (gf_hbm, gf_v), (gs_hbm, gs_v))
        )
    ]
    early_in = [load(master_hbm.at[:, pl.ds(64 * h, EARLY), :], early_v.at[:, 2 * me + h], in_sem.at[10 + h]) for h in (0, 1)]
    for c in (*fac_in, ccot_in, logs_in, cot_in[0], x_in[0], cot_in[1], *x_in[1:], cot_in[2], *early_in, *rest_in):
        c.start()

    barrier = pltpu.get_barrier_semaphore()

    @pl.loop(1, FS)
    def _(d):
        pl.semaphore_signal(barrier, inc=1, device_id={"fs": (me + d) % FS}, device_id_type=MESH)

    @pl.loop(1, TP)
    def _(d):
        pl.semaphore_signal(barrier, inc=1, device_id={"tp": (tp + d) % TP}, device_id_type=MESH)

    def put(src, dst, send, recv, to):
        return pltpu.make_async_remote_copy(src, dst, send, recv, device_id=to, device_id_type=MESH)

    def to_peers(src, dst, k):
        @pl.loop(1, FS)
        def _(d):
            peer = (me + d) % FS
            put(src(peer), dst, p_send.at[k], p_recv.at[k], {"fs": peer}).start()

    def from_peers(ref, k):
        ref = ref.at[pl.ds(0, FS - 1)]
        put(ref, ref, p_send.at[k], p_recv.at[k], {"fs": (me + 1) % FS}).wait_recv()

    def sent(ref, k):
        ref = ref.at[pl.ds(0, FS - 1)]
        put(ref, ref, p_send.at[k], p_recv.at[k], {"fs": (me + 1) % FS}).wait_send()

    me_x, me_z = me % RING, me // RING
    at = ((me_x, me_z), (me_z, me_x))

    def device(half, first, second):
        return {"fs": second * RING + first if half == 0 else first * RING + second}

    def turn(a, d):
        return (a + d) % RING

    def rows(start, size):
        return pl.ds(pl.multiple_of(start, 8), size)

    def swap(r, phase):
        for half in (0, 1):
            p, q = at[half]
            for d in (1, 3, 2):
                if phase == 0:
                    to = (turn(p, d), q)
                    src = lowp_v.at[r, rows(128 * half + 32 * to[0], 32)]
                    dst = sum_a.at[r, half, d - 1]
                elif phase == 1:
                    to = (p, turn(q, d))
                    src = sum_b.at[r, half, rows(8 * to[1], 8)]
                    dst = sum_c.at[r, half, d - 1]
                elif phase == 2:
                    to = (p, turn(q, d))
                    src = dst = low_v.at[r, rows(128 * half + 32 * p + 8 * q, 8)]
                else:
                    to = (turn(p, d), q)
                    src = dst = low_v.at[r, rows(128 * half + 32 * p, 32)]
                put(src, dst, s_send.at[r], s_recv.at[r, phase], device(half, *to)).start()

    def whole(r, phase):
        ref = (sum_a.at[r], sum_c.at[r], low_v.at[r, pl.ds(0, 48)], low_v.at[r, pl.ds(0, 192)])[phase]
        return put(ref, ref, s_send.at[r], s_recv.at[r, phase], {"fs": (me + 1) % FS})

    def second_sum(r):
        whole(r, 0).wait_recv()
        for half in (0, 1):
            p, q = at[half]
            got = sum_a[r, half]
            sum_b[r, half] = lowp_v[r, rows(128 * half + 32 * p, 32)] + got[0] + got[1] + got[2]
        swap(r, 1)

    def first_spread(r):
        whole(r, 1).wait_recv()
        for half in (0, 1):
            p, q = at[half]
            got = sum_c[r, half]
            low_v[r, rows(128 * half + 32 * p + 8 * q, 8)] = sum_b[r, half, rows(8 * q, 8)] + got[0] + got[1] + got[2]
        swap(r, 2)

    def second_spread(r):
        whole(r, 2).wait_recv()
        swap(r, 3)

    ccot_in.wait()
    logs_in.wait()
    small = lax.broadcasted_iota(jnp.int32, (8, 128), 1)
    sums = jnp.sum(ccot_v[...], axis=1, keepdims=True)
    ends = logs_v[:, TOK - 128 :][:, 127:128]
    message = jnp.where(small < 32, sums[:8], sums[8:])
    message = jnp.where(small < 64, message, ends[:8])
    gx_v[me] = jnp.where(small < 96, message, ends[8:])

    facs = [
        Gather(
            me,
            lambda i, h, r=r: fac_v.at[r, 2 * i + h, core],
            lambda n, r=r: fac_v.at[r, pl.ds(0, n), core],
            f_send.at[r],
            f_recv.at[r],
            True,
        )
        for r in range(ROLES)
    ]
    fac_in[0].wait()
    fac_in[1].wait()
    pl.semaphore_wait(barrier, FS + TP - 2)
    to_peers(lambda peer: gx_v.at[me], gx_v.at[me], 0)
    for r in range(ROLES):
        facs[r].first()

    lane = lax.broadcasted_iota(jnp.int32, (HEADS, TOK), 1)
    later = ccot_v[...]
    by = 1
    while by < TOK:
        later = later + jnp.where(lane < TOK - by, pltpu.roll(later, TOK - by, 1), 0.0)
        by *= 2
    later_v[...] = later
    logs = logs_v[...]
    gate_v[...] = minus_expm1(logs - pltpu.roll(logs, 1, 1))

    def across(r, side):
        return pltpu.make_async_remote_copy(
            fac_v.at[r, :, side], fac_v.at[r, :, side], d_send.at[r], d_recv.at[r],
            device_id={"tp": tp + 1 - 2 * core}, device_id_type=MESH,
        )

    early = Gather(
        me, lambda i, h: early_v.at[:, 2 * i + h], lambda n: early_v.at[:, pl.ds(0, n)], e_send.at[0], e_recv
    )

    def early_first():
        for c in early_in:
            c.wait()
        early.first()

    def other_gates(side):
        ref = gfull_v.at[:, side]
        return put(ref, ref, d_send.at[ROLES], d_recv.at[ROLES], {"tp": tp + 1 - 2 * core})

    def turned(r, n):
        span = pl.ds(pl.multiple_of(TURN * n, TURN), TURN)
        lhs_v[r % 2, 0:COLS, span] = cot_v[r, span, :].T

    def contract(r):
        fac = fac_v[r].reshape(DIM, RANK)
        both = jnp.dot(grad_v[r], fac, preferred_element_type=F32)
        lowp_v[r] = (both[:COLS] + both[COLS:]).T
        swap(r, 0)

    def finish(r):
        low = low_v[r]
        first = BETA_ONE * fm_v[r] + (1.0 - BETA_ONE) * low
        second = BETA_TWO * sm_v[r] + (1.0 - BETA_TWO) * low * low
        first_ref[r] = first
        second_ref[r] = second
        direction = first * lax.rsqrt(second)
        own = fac_v[r, pl.ds(2 * me, 2)].reshape(128, RANK)
        dir_v[r] = jnp.concatenate(halves(direction), axis=1)
        both = jnp.dot(own, dir_v[r], preferred_element_type=F32)
        prod_v[r] = both[:, :COLS] + both[:, COLS:]

    def early_rows(r, scale):
        fac = fac_v[r, :, 0, 0:EARLY, :].reshape(2 * FS * EARLY, RANK)
        both = jnp.dot(fac, dir_v[r], preferred_element_type=F32)
        prod = (both[:, :COLS] + both[:, COLS:]).reshape(2 * FS, EARLY, COLS)
        copy_ref[r, :, 0:EARLY, :] = (early_v[r] - LEARN * (scale * prod)).astype(BF16)

    cot_in[0].wait()

    @pl.loop(0, BLOCKS)
    def _(n):
        turned(0, n)

    def handed(r):
        facs[r].last()
        across(r, core).start()

    def joined(r):
        across(r, 1 - core).wait_recv()
        contract(r)

    events = ((1, facs[0].second), (2, facs[1].second), (3, facs[2].second),), ((0, facs[0].third), (1, facs[1].third), (2, facs[2].third), (3, functools.partial(handed, 0)), (3, early_first),), ((0, functools.partial(handed, 1)), (1, functools.partial(handed, 2)), (1, functools.partial(joined, 0)), (2, functools.partial(joined, 1)),)

    for r in range(ROLES):
        height = COLS + HEADS if r == 1 else COLS

        @pl.loop(0, BLOCKS)
        def _(n):
            if r == 0:
                load(x_hbm.at[:, pl.ds(pl.multiple_of(BLOCK * n, BLOCK), BLOCK)], x_v.at[n], x_sem.at[n]).wait()
            if r + 1 < ROLES:
                pl.when(n == 0)(cot_in[r + 1].wait)
                turned(r + 1, n)
            grad = jnp.dot(lhs_v[r % 2, 0:height, :], x_v[n], preferred_element_type=F32)
            upper, lower = halves(grad[:COLS])
            span = pl.ds(pl.multiple_of(BLOCK * n, BLOCK), BLOCK)
            grad_v[r, 0:COLS, span] = upper
            grad_v[r, COLS:, span] = lower
            if r == 1:
                for i in range(BLOCK // 128):
                    for c in (0, 1):
                        gp_v[(BLOCK // 128) * n + i, c] = grad[COLS + 8 * c : COLS + 8 * c + 8, 128 * i : 128 * i + 128]
            for event, work in events[r]:
                pl.when(n == event)(work)

        if r == 0:
            from_peers(gx_v, 0)
            carried = jnp.zeros((8, 128), F32)
            edge = jnp.zeros((8, 128), F32)
            for i in range(FS):
                message = gx_v[i]
                carried = carried + jnp.where(i > me, message, 0.0)
                edge = edge + jnp.where(i == me - 1, message, 0.0)
            carried = jnp.concatenate([carried[:, 0:1], carried[:, 32:33]], axis=0)
            edge = jnp.concatenate([edge[:, 64:65], edge[:, 96:97]], axis=0)
            lhs_v[1, COLS:, :] = ((later_v[...] + carried) * gate_v[...]).astype(BF16)
            start = logs_v[:, 0:128]
            start = start - jnp.where(lane[:, 0:128] == 0, edge, pltpu.roll(start, 1, 1))
            lhs_v[1, COLS:, 0:128] = ((later_v[:, 0:128] + carried) * minus_expm1(start)).astype(BF16)
        if r == 1:
            to_peers(lambda peer: gp_v.at[peer, core], grs_v.at[me], 1)
            grs_v[me] = gp_v[me, core]

    joined(2)
    for c in rest_in:
        c.wait()

    def slice_squares(r):
        squares = jnp.zeros((8, COLS), F32)
        for half in (0, 1):
            p, q = at[half]
            own = rows(128 * half + 32 * p + 8 * q, 8)
            low = low_v[r, own]
            first = BETA_ONE * fm_v[r, own] + (1.0 - BETA_ONE) * low
            second = BETA_TWO * sm_v[r, own] + (1.0 - BETA_TWO) * low * low
            direction = first * lax.rsqrt(second)
            squares = squares + direction * direction
        return jnp.sum(squares[:, :128] + squares[:, 128:], axis=0, keepdims=True)

    from_peers(grs_v, 1)
    gfull_v[me, core] = jnp.sum(grs_v[...], axis=0)
    second_sum(0)
    second_sum(1)
    second_sum(2)
    early.second(True, (1, 3))
    first_spread(0)
    first_spread(1)
    first_spread(2)

    ss_v[tp] = slice_squares(0) + slice_squares(1) + slice_squares(2)

    @pl.loop(1, TP)
    def _(d):
        put(ss_v.at[tp], ss_v.at[tp], ss_sem.at[0], ss_sem.at[1], {"tp": (tp + d) % TP}).start()

    squares = put(ss_v.at[pl.ds(0, TP - 1)], ss_v.at[pl.ds(0, TP - 1)], ss_sem.at[0], ss_sem.at[1], {"tp": (tp + 1) % TP})
    early.second(False, (2,))
    to_peers(lambda peer: gfull_v.at[me, core], gfull_v.at[me, core], 2)
    second_spread(0)
    second_spread(1)
    squares.wait_recv()
    st_v[me] = jnp.sum(ss_v[...], axis=0)
    to_peers(lambda peer: st_v.at[me], st_v.at[me], 3)
    second_spread(2)
    early.third()
    whole(0, 3).wait_recv()
    finish(0)
    whole(1, 3).wait_recv()
    finish(1)
    whole(2, 3).wait_recv()
    finish(2)

    from_peers(st_v, 3)
    total = jnp.sum(jnp.sum(st_v[...], axis=0), keepdims=True)
    scale = lax.rsqrt(total * (1.0 / (ROLES * RANK * COLS * TP)) + 1e-06)
    copies = [
        Gather(
            me,
            lambda i, h, r=r: copy_ref.at[r, 2 * i + h, pl.ds(EARLY, 64 - EARLY)],
            lambda n, r=r: copy_ref.at[r, pl.ds(0, n), pl.ds(EARLY, 64 - EARLY)],
            c_send.at[r],
            c_recv.at[r],
        )
        for r in range(ROLES)
    ]
    for r in range(ROLES):
        step = scale * prod_v[r]
        new = master_v[r] - LEARN * step
        step_ref[r] = step
        new_ref[r] = new
        copy_ref[r, pl.ds(2 * me, 2), EARLY:, :] = new.astype(BF16).reshape(2, 64, COLS)[:, EARLY:, :]
        copies[r].first()

    from_peers(grs_v, 2)
    other_gates(core).start()
    other_gates(1 - core).wait_recv()
    for i in range(FS):
        cut = slice(128 * i, 128 * i + 128)
        gate = gfull_v[i].reshape(HEADS, 128)
        first = BETA_ONE * gf_v[:, cut] + (1.0 - BETA_ONE) * gate
        second = BETA_TWO * gs_v[:, cut] + (1.0 - BETA_TWO) * gate * gate
        new = gm_v[:, cut] - LEARN * (first * lax.rsqrt(second))
        gfirst_ref[:, cut] = first
        gsecond_ref[:, cut] = second
        gnew_ref[:, cut] = new
        gcopy_ref[:, cut] = new.astype(BF16)
    squares.wait_send()
    for r in range(ROLES):
        across(r, core).wait_send()
        put(lowp_v.at[pl.ds(0, 2), pl.ds(0, 240)], lowp_v.at[pl.ds(0, 2), pl.ds(0, 240)], s_send.at[r], s_recv.at[r, 0], {"fs": (me + 1) % FS}).wait_send()
    sent(gx_v, 0)
    sent(grs_v, 1)
    sent(grs_v, 2)
    other_gates(core).wait_send()
    sent(st_v, 3)
    for r in range(ROLES):
        facs[r].drain()

    early.last()
    for r in range(ROLES):
        early_rows(r, scale)
    early.drain()

    for step in ("second", "third", "last", "drain"):
        for gather in copies:
            getattr(gather, step)()


def written(*refs):
    copies = [pltpu.make_async_copy(refs[i], refs[9 + i], refs[18].at[i]) for i in range(9)]
    for c in copies:
        c.start()
    for c in copies:
        c.wait()


def local(*args):
    shapes = (
        ((ROLES, 128, COLS), F32),
        ((ROLES, 128, COLS), F32),
        ((ROLES, 2 * FS, 64, COLS), BF16),
        ((ROLES, RANK, COLS), F32),
        ((ROLES, RANK, COLS), F32),
        ((HEADS, DIM), F32),
        ((HEADS, DIM), BF16),
        ((HEADS, DIM), F32),
        ((HEADS, DIM), F32),
    )
    vmem, dma = pltpu.VMEM, pltpu.SemaphoreType.DMA
    gates = vmem((HEADS, DIM), F32)
    moments = vmem((ROLES, RANK, COLS), F32)
    outs = pl.pallas_call(
        kernel,
        out_shape=[vmem(s, d) for s, d in shapes],
        in_specs=[pl.BlockSpec(memory_space=pl.ANY)] * 11,
        out_specs=[pl.BlockSpec(memory_space=vmem)] * 9,
        scratch_shapes=[
            vmem((BLOCKS, TOK, BLOCK), BF16),
            vmem((ROLES, TOK, COLS), BF16),
            vmem((HEADS, TOK), F32),
            vmem((HEADS, TOK), F32),
            vmem((ROLES, 128, COLS), F32),
            vmem((ROLES, 2 * FS, 2, 32, RANK), BF16),
            moments, moments, gates, gates, gates,
            vmem((2, COLS + HEADS, TOK), BF16),
            vmem((ROLES, 2 * COLS, DIM), BF16),
            vmem((HEADS, TOK), F32),
            vmem((HEADS, TOK), F32),
            vmem((FS, 8, 128), F32),
            moments,
            vmem((ROLES, 2, 3, 32, COLS), F32),
            vmem((ROLES, 2, 32, COLS), F32),
            vmem((ROLES, 2, 3, 8, COLS), F32),
            moments,
            vmem((FS, 2, 8, 128), F32),
            vmem((FS, 8, 128), F32),
            vmem((FS, 2, 8, 128), F32),
            vmem((ROLES, 128, COLS), F32),
            vmem((TP, 1, 128), F32),
            vmem((FS, 1, 128), F32),
            vmem((ROLES, 2 * FS, EARLY, COLS), F32),
            vmem((ROLES, RANK, 2 * COLS), BF16),
            dma((12,)), dma((BLOCKS,)), dma((ROLES,)),
            dma((4,)), dma((4,)), dma((ROLES,)), dma((ROLES, 4)), dma((2,)),
            dma((ROLES,)), dma((ROLES, 3)), dma((ROLES + 1,)), dma((ROLES + 1,)), dma((ROLES,)), dma((ROLES, 8)),
            dma((1,)), dma((8,)),
        ],
        compiler_params=pltpu.CompilerParams(
            collective_id=0, has_side_effects=True, vmem_limit_bytes=57 * 1024 * 1024
        ),
    )(*args)
    outs = pl.pallas_call(
        written,
        out_shape=[jax.ShapeDtypeStruct(s, d) for s, d in shapes],
        in_specs=[pl.BlockSpec(memory_space=vmem)] * 9,
        out_specs=[pl.BlockSpec(memory_space=pl.ANY)] * 9,
        scratch_shapes=[dma((9,))],
        compiler_params=pltpu.CompilerParams(vmem_limit_bytes=1024 * 1024),
    )(*(pltpu.with_memory_space_constraint(o, pltpu.VMEM) for o in outs))
    outs = list(outs)
    outs[2] = outs[2].reshape(ROLES, DIM, COLS)
    return tuple(outs)


def solution(mesh):
    placed = (
        P("fs", None),
        P(None, "fs", "tp"),
        P(None, "fs"),
        P(None, "fs"),
        P(None, "fs", "tp"),
        P(None, "fs", None),
        P(None, None, "tp"),
        P(None, None, "tp"),
        P(),
        P(),
        P(),
    )
    return jax.shard_map(
        local,
        mesh=mesh,
        in_specs=placed,
        out_specs=(
            P(None, "fs", "tp"),
            P(None, "fs", "tp"),
            P(None, None, "tp"),
            P(None, None, "tp"),
            P(None, None, "tp"),
            P(),
            P(),
            P(),
            P(),
        ),
        check_vma=False,
    )
```

```python
import functools

import jax
import jax.numpy as jnp
from jax import lax
from jax.experimental import pallas as pl
from jax.experimental.pallas import tpu as pltpu
from jax.sharding import PartitionSpec as P

BETA_ONE = 0.8
BETA_TWO = 0.9
LEARN = 0.001
MESH = pl.DeviceIdType.MESH
F32, BF16 = jnp.float32, jnp.bfloat16

FS, TP, RING = 16, 8, 4
ROLES, TOK, DIM, COLS, RANK, HEADS = 3, 3072, 2048, 256, 256, 16
BLOCK = 512
BLOCKS = DIM // BLOCK
EARLY = 16
TURN = TOK // BLOCKS


def minus_expm1(x):
    series = jnp.ones_like(x)
    for n in range(9, 1, -1):
        series = 1.0 + x * (1.0 / n) * series
    return jnp.where(jnp.abs(x) < 0.5, -x * series, 1.0 - jnp.exp(x))


def halves(x):
    upper = x.astype(BF16)
    return upper, (x - upper.astype(F32)).astype(BF16)


class Gather:
    def __init__(self, me, piece, many, send, recv, coarse=False):
        self.me, self.piece, self.many, self.send, self.recv, self.coarse = me, piece, many, send, recv, coarse
        x, z = me % RING, me // RING
        self.at = ((x, z), (z, x))

    def name(self, half, first, second):
        return second * RING + first if half == 0 else first * RING + second

    def sem(self, index):
        if index < 3:
            return self.recv.at[1 if self.coarse else 1 + index]
        e, kind = divmod(index - 3, 3)
        if kind == (0 if e < 2 else 1):
            return self.recv.at[(1 if e == 0 else 2) if self.coarse else 4 + e]
        return self.recv.at[0]

    def copy(self, half, index):
        p, q = self.at[half]
        turn = lambda a, b: (a + b + RING) % RING
        if index < 3:
            d = index + 1
            out, to = (p, q), (turn(p, d), q)
        else:
            e, kind = divmod(index - 3, 3)
            first = turn(p, -e)
            if kind == 0:
                out, to = (first, q), (p, turn(q, 1))
            elif kind == 1:
                out, to = (first, q), (p, turn(q, -1))
            elif e < 2:
                out, to = (first, turn(q, -1)), (p, turn(q, 1))
            else:
                out, to = (first, turn(q, 1)), (p, turn(q, -1))
        ref = self.piece(self.name(half, *out), half)
        return pltpu.make_async_remote_copy(
            ref, ref, self.send, self.sem(index), device_id={"fs": self.name(half, *to)}, device_id_type=MESH
        )

    def start(self, index):
        for half in (0, 1):
            self.copy(half, index).start()

    def arrived(self, index):
        self.whole(2, self.sem(index)).wait_recv()

    def first(self):
        for index in (1, 0, 2, 3, 4):
            self.start(index)

    def second(self, own=True, behind=(1, 3, 2)):
        if self.coarse:
            self.whole(8, self.recv.at[1]).wait_recv()
        if own:
            if not self.coarse:
                self.arrived(3)
            self.start(5)
        for e in behind:
            if not self.coarse:
                self.arrived(e - 1)
            self.start(3 + 3 * e)
            self.start(4 + 3 * e)

    def third(self):
        if self.coarse:
            self.whole(6, self.recv.at[2]).wait_recv()
        for e in (1, 3, 2):
            if not self.coarse:
                self.arrived(3 + 3 * e if e < 2 else 4 + 3 * e)
            self.start(5 + 3 * e)

    def whole(self, n, sem):
        ref = self.many(n)
        return pltpu.make_async_remote_copy(
            ref, ref, self.send, sem, device_id={"fs": (self.me + 1) % FS}, device_id_type=MESH
        )

    def last(self):
        self.whole(16, self.recv.at[0]).wait_recv()

    def drain(self):
        self.whole(30, self.recv.at[0]).wait_send()


def kernel(
    x_hbm, cot_hbm, logs_hbm, ccot_hbm, master_hbm, factors_hbm, first_hbm, second_hbm, gm_hbm, gf_hbm, gs_hbm,
    step_ref, new_ref, copy_ref, first_ref, second_ref, gnew_ref, gcopy_ref, gfirst_ref, gsecond_ref,
    x_v, cot_v, logs_v, ccot_v, master_v, fac_v, fm_v, sm_v, gm_v, gf_v, gs_v,
    lhs_v, grad_v, later_v, gate_v, gx_v, lowp_v, sum_a, sum_b, sum_c, low_v, gp_v, grs_v, gfull_v, prod_v, ss_v, st_v, early_v, dir_v,
    in_sem, x_sem, cot_sem, p_send, p_recv, s_send, s_recv, ss_sem, f_send, f_recv, d_send, d_recv, c_send, c_recv, e_send, e_recv,
):
    me, tp = lax.axis_index("fs"), lax.axis_index("tp")
    core = tp % 2

    barrier = pltpu.get_barrier_semaphore()

    @pl.loop(1, FS)
    def _(d):
        pl.semaphore_signal(barrier, inc=1, device_id={"fs": (me + d) % FS}, device_id_type=MESH)

    @pl.loop(1, TP)
    def _(d):
        pl.semaphore_signal(barrier, inc=1, device_id={"tp": (tp + d) % TP}, device_id_type=MESH)

    def load(src, dst, sem):
        return pltpu.make_async_copy(src, dst, sem)

    fac_in = [
        load(factors_hbm.at[:, pl.ds(pl.multiple_of(64 * h + 32 * core, 32), 32), :], fac_v.at[:, 2 * me + h, core], in_sem.at[h])
        for h in (0, 1)
    ]
    logs_in = load(logs_hbm, logs_v, in_sem.at[2])
    ccot_in = load(ccot_hbm, ccot_v, in_sem.at[3])
    cot_in = [load(cot_hbm.at[r], cot_v.at[r], cot_sem.at[r]) for r in range(ROLES)]
    x_in = [load(x_hbm.at[:, pl.ds(BLOCK * n, BLOCK)], x_v.at[n], x_sem.at[n]) for n in range(BLOCKS)]
    rest_in = [
        load(s, d, in_sem.at[4 + i])
        for i, (s, d) in enumerate(
            ((first_hbm, fm_v), (second_hbm, sm_v), (master_hbm, master_v), (gm_hbm, gm_v), (gf_hbm, gf_v), (gs_hbm, gs_v))
        )
    ]
    early_in = [load(master_hbm.at[:, pl.ds(64 * h, EARLY), :], early_v.at[:, 2 * me + h], in_sem.at[10 + h]) for h in (0, 1)]
    for c in (*fac_in, ccot_in, logs_in, cot_in[0], x_in[0], cot_in[1], *x_in[1:], cot_in[2], *early_in, *rest_in):
        c.start()

    def put(src, dst, send, recv, to):
        return pltpu.make_async_remote_copy(src, dst, send, recv, device_id=to, device_id_type=MESH)

    def to_peers(src, dst, k):
        @pl.loop(1, FS)
        def _(d):
            peer = (me + d) % FS
            put(src(peer), dst, p_send.at[k], p_recv.at[k], {"fs": peer}).start()

    def from_peers(ref, k):
        ref = ref.at[pl.ds(0, FS - 1)]
        put(ref, ref, p_send.at[k], p_recv.at[k], {"fs": (me + 1) % FS}).wait_recv()

    def sent(ref, k):
        ref = ref.at[pl.ds(0, FS - 1)]
        put(ref, ref, p_send.at[k], p_recv.at[k], {"fs": (me + 1) % FS}).wait_send()

    me_x, me_z = me % RING, me // RING
    at = ((me_x, me_z), (me_z, me_x))

    def device(half, first, second):
        return {"fs": second * RING + first if half == 0 else first * RING + second}

    def turn(a, d):
        return (a + d) % RING

    def rows(start, size):
        return pl.ds(pl.multiple_of(start, 8), size)

    def swap(r, phase):
        for half in (0, 1):
            p, q = at[half]
            for d in (1, 3, 2):
                if phase == 0:
                    to = (turn(p, d), q)
                    src = lowp_v.at[r, rows(128 * half + 32 * to[0], 32)]
                    dst = sum_a.at[r, half, d - 1]
                elif phase == 1:
                    to = (p, turn(q, d))
                    src = sum_b.at[r, half, rows(8 * to[1], 8)]
                    dst = sum_c.at[r, half, d - 1]
                elif phase == 2:
                    to = (p, turn(q, d))
                    src = dst = low_v.at[r, rows(128 * half + 32 * p + 8 * q, 8)]
                else:
                    to = (turn(p, d), q)
                    src = dst = low_v.at[r, rows(128 * half + 32 * p, 32)]
                put(src, dst, s_send.at[r], s_recv.at[r, phase], device(half, *to)).start()

    def whole(r, phase):
        ref = (sum_a.at[r], sum_c.at[r], low_v.at[r, pl.ds(0, 48)], low_v.at[r, pl.ds(0, 192)])[phase]
        return put(ref, ref, s_send.at[r], s_recv.at[r, phase], {"fs": (me + 1) % FS})

    def second_sum(r):
        whole(r, 0).wait_recv()
        for half in (0, 1):
            p, q = at[half]
            got = sum_a[r, half]
            sum_b[r, half] = lowp_v[r, rows(128 * half + 32 * p, 32)] + got[0] + got[1] + got[2]
        swap(r, 1)

    def first_spread(r):
        whole(r, 1).wait_recv()
        for half in (0, 1):
            p, q = at[half]
            got = sum_c[r, half]
            low_v[r, rows(128 * half + 32 * p + 8 * q, 8)] = sum_b[r, half, rows(8 * q, 8)] + got[0] + got[1] + got[2]
        swap(r, 2)

    def second_spread(r):
        whole(r, 2).wait_recv()
        swap(r, 3)

    ccot_in.wait()
    logs_in.wait()
    small = lax.broadcasted_iota(jnp.int32, (8, 128), 1)
    sums = jnp.sum(ccot_v[...], axis=1, keepdims=True)
    ends = logs_v[:, TOK - 128 :][:, 127:128]
    message = jnp.where(small < 32, sums[:8], sums[8:])
    message = jnp.where(small < 64, message, ends[:8])
    gx_v[me] = jnp.where(small < 96, message, ends[8:])

    facs = [
        Gather(
            me,
            lambda i, h, r=r: fac_v.at[r, 2 * i + h, core],
            lambda n, r=r: fac_v.at[r, pl.ds(0, n), core],
            f_send.at[r],
            f_recv.at[r],
            True,
        )
        for r in range(ROLES)
    ]
    fac_in[0].wait()
    fac_in[1].wait()
    pl.semaphore_wait(barrier, FS + TP - 2)
    to_peers(lambda peer: gx_v.at[me], gx_v.at[me], 0)
    for r in range(ROLES):
        facs[r].first()

    lane = lax.broadcasted_iota(jnp.int32, (HEADS, TOK), 1)
    later = ccot_v[...]
    by = 1
    while by < TOK:
        later = later + jnp.where(lane < TOK - by, pltpu.roll(later, TOK - by, 1), 0.0)
        by *= 2
    later_v[...] = later
    logs = logs_v[...]
    gate_v[...] = minus_expm1(logs - pltpu.roll(logs, 1, 1))

    def across(r, side):
        return pltpu.make_async_remote_copy(
            fac_v.at[r, :, side], fac_v.at[r, :, side], d_send.at[r], d_recv.at[r],
            device_id={"tp": tp + 1 - 2 * core}, device_id_type=MESH,
        )

    early = Gather(
        me, lambda i, h: early_v.at[:, 2 * i + h], lambda n: early_v.at[:, pl.ds(0, n)], e_send.at[0], e_recv
    )

    def early_first():
        for c in early_in:
            c.wait()
        early.first()

    def other_gates(side):
        ref = gfull_v.at[:, side]
        return put(ref, ref, d_send.at[ROLES], d_recv.at[ROLES], {"tp": tp + 1 - 2 * core})

    def turned(r, n):
        span = pl.ds(pl.multiple_of(TURN * n, TURN), TURN)
        lhs_v[r % 2, 0:COLS, span] = cot_v[r, span, :].T

    def contract(r):
        fac = fac_v[r].reshape(DIM, RANK)
        both = jnp.dot(grad_v[r], fac, preferred_element_type=F32)
        lowp_v[r] = (both[:COLS] + both[COLS:]).T
        swap(r, 0)

    def finish(r):
        low = low_v[r]
        first = BETA_ONE * fm_v[r] + (1.0 - BETA_ONE) * low
        second = BETA_TWO * sm_v[r] + (1.0 - BETA_TWO) * low * low
        first_ref[r] = first
        second_ref[r] = second
        direction = first * lax.rsqrt(second)
        own = fac_v[r, pl.ds(2 * me, 2)].reshape(128, RANK)
        dir_v[r] = jnp.concatenate(halves(direction), axis=1)
        both = jnp.dot(own, dir_v[r], preferred_element_type=F32)
        prod_v[r] = both[:, :COLS] + both[:, COLS:]

    def early_rows(r, scale):
        fac = fac_v[r, :, 0, 0:EARLY, :].reshape(2 * FS * EARLY, RANK)
        both = jnp.dot(fac, dir_v[r], preferred_element_type=F32)
        prod = (both[:, :COLS] + both[:, COLS:]).reshape(2 * FS, EARLY, COLS)
        copy_ref[r, :, 0:EARLY, :] = (early_v[r] - LEARN * (scale * prod)).astype(BF16)

    cot_in[0].wait()

    @pl.loop(0, BLOCKS)
    def _(n):
        turned(0, n)

    def handed(r):
        facs[r].last()
        across(r, core).start()

    def joined(r):
        across(r, 1 - core).wait_recv()
        contract(r)

    events = ((1, facs[0].second), (2, facs[1].second), (3, facs[2].second),), ((0, facs[0].third), (1, facs[1].third), (2, facs[2].third), (3, functools.partial(handed, 0)), (3, early_first),), ((0, functools.partial(handed, 1)), (1, functools.partial(handed, 2)), (1, functools.partial(joined, 0)), (2, functools.partial(joined, 1)), (3, functools.partial(joined, 2)),)

    for r in range(ROLES):
        height = COLS + HEADS if r == 1 else COLS

        @pl.loop(0, BLOCKS)
        def _(n):
            if r == 0:
                load(x_hbm.at[:, pl.ds(pl.multiple_of(BLOCK * n, BLOCK), BLOCK)], x_v.at[n], x_sem.at[n]).wait()
            if r + 1 < ROLES:
                pl.when(n == 0)(cot_in[r + 1].wait)
                turned(r + 1, n)
            grad = jnp.dot(lhs_v[r % 2, 0:height, :], x_v[n], preferred_element_type=F32)
            upper, lower = halves(grad[:COLS])
            span = pl.ds(pl.multiple_of(BLOCK * n, BLOCK), BLOCK)
            grad_v[r, 0:COLS, span] = upper
            grad_v[r, COLS:, span] = lower
            if r == 1:
                for i in range(BLOCK // 128):
                    for c in (0, 1):
                        gp_v[(BLOCK // 128) * n + i, c] = grad[COLS + 8 * c : COLS + 8 * c + 8, 128 * i : 128 * i + 128]
            for event, work in events[r]:
                pl.when(n == event)(work)

        if r == 0:
            from_peers(gx_v, 0)
            carried = jnp.zeros((8, 128), F32)
            edge = jnp.zeros((8, 128), F32)
            for i in range(FS):
                message = gx_v[i]
                carried = carried + jnp.where(i > me, message, 0.0)
                edge = edge + jnp.where(i == me - 1, message, 0.0)
            carried = jnp.concatenate([carried[:, 0:1], carried[:, 32:33]], axis=0)
            edge = jnp.concatenate([edge[:, 64:65], edge[:, 96:97]], axis=0)
            lhs_v[1, COLS:, :] = ((later_v[...] + carried) * gate_v[...]).astype(BF16)
            start = logs_v[:, 0:128]
            start = start - jnp.where(lane[:, 0:128] == 0, edge, pltpu.roll(start, 1, 1))
            lhs_v[1, COLS:, 0:128] = ((later_v[:, 0:128] + carried) * minus_expm1(start)).astype(BF16)
        if r == 1:
            to_peers(lambda peer: gp_v.at[peer, core], grs_v.at[me], 1)
            grs_v[me] = gp_v[me, core]

    for c in rest_in:
        c.wait()

    def slice_squares(r):
        squares = jnp.zeros((8, COLS), F32)
        for half in (0, 1):
            p, q = at[half]
            own = rows(128 * half + 32 * p + 8 * q, 8)
            low = low_v[r, own]
            first = BETA_ONE * fm_v[r, own] + (1.0 - BETA_ONE) * low
            second = BETA_TWO * sm_v[r, own] + (1.0 - BETA_TWO) * low * low
            direction = first * lax.rsqrt(second)
            squares = squares + direction * direction
        return jnp.sum(squares[:, :128] + squares[:, 128:], axis=0, keepdims=True)

    from_peers(grs_v, 1)
    gfull_v[me, core] = jnp.sum(grs_v[...], axis=0)
    second_sum(0)
    second_sum(1)
    second_sum(2)
    first_spread(0)
    first_spread(1)
    early.second(True, (1, 3))
    first_spread(2)

    ss_v[tp] = slice_squares(0) + slice_squares(1) + slice_squares(2)

    @pl.loop(1, TP)
    def _(d):
        put(ss_v.at[tp], ss_v.at[tp], ss_sem.at[0], ss_sem.at[1], {"tp": (tp + d) % TP}).start()

    squares = put(ss_v.at[pl.ds(0, TP - 1)], ss_v.at[pl.ds(0, TP - 1)], ss_sem.at[0], ss_sem.at[1], {"tp": (tp + 1) % TP})
    second_spread(0)
    second_spread(1)
    early.second(False, (2,))
    squares.wait_recv()
    st_v[me] = jnp.sum(ss_v[...], axis=0)
    to_peers(lambda peer: st_v.at[me], st_v.at[me], 3)
    second_spread(2)
    to_peers(lambda peer: gfull_v.at[me, core], gfull_v.at[me, core], 2)
    whole(0, 3).wait_recv()
    finish(0)
    whole(1, 3).wait_recv()
    finish(1)
    early.third()
    whole(2, 3).wait_recv()
    finish(2)

    from_peers(st_v, 3)
    total = jnp.sum(jnp.sum(st_v[...], axis=0), keepdims=True)
    scale = lax.rsqrt(total * (1.0 / (ROLES * RANK * COLS * TP)) + 1e-06)
    copies = [
        Gather(
            me,
            lambda i, h, r=r: copy_ref.at[r, 2 * i + h, pl.ds(EARLY, 64 - EARLY)],
            lambda n, r=r: copy_ref.at[r, pl.ds(0, n), pl.ds(EARLY, 64 - EARLY)],
            c_send.at[r],
            c_recv.at[r],
        )
        for r in range(ROLES)
    ]
    for r in range(ROLES):
        step = scale * prod_v[r]
        new = master_v[r] - LEARN * step
        step_ref[r] = step
        new_ref[r] = new
        copy_ref[r, pl.ds(2 * me, 2), EARLY:, :] = new.astype(BF16).reshape(2, 64, COLS)[:, EARLY:, :]
        copies[r].first()

    from_peers(grs_v, 2)
    other_gates(core).start()
    other_gates(1 - core).wait_recv()
    for i in range(FS):
        cut = slice(128 * i, 128 * i + 128)
        gate = gfull_v[i].reshape(HEADS, 128)
        first = BETA_ONE * gf_v[:, cut] + (1.0 - BETA_ONE) * gate
        second = BETA_TWO * gs_v[:, cut] + (1.0 - BETA_TWO) * gate * gate
        new = gm_v[:, cut] - LEARN * (first * lax.rsqrt(second))
        gfirst_ref[:, cut] = first
        gsecond_ref[:, cut] = second
        gnew_ref[:, cut] = new
        gcopy_ref[:, cut] = new.astype(BF16)
    squares.wait_send()
    for r in range(ROLES):
        across(r, core).wait_send()
        put(lowp_v.at[pl.ds(0, 2), pl.ds(0, 240)], lowp_v.at[pl.ds(0, 2), pl.ds(0, 240)], s_send.at[r], s_recv.at[r, 0], {"fs": (me + 1) % FS}).wait_send()
    sent(gx_v, 0)
    sent(grs_v, 1)
    sent(grs_v, 2)
    other_gates(core).wait_send()
    sent(st_v, 3)
    for r in range(ROLES):
        facs[r].drain()

    early.last()
    for r in range(ROLES):
        early_rows(r, scale)
    early.drain()

    for step in ("second", "third", "last", "drain"):
        for gather in copies:
            getattr(gather, step)()


def written(*refs):
    copies = [pltpu.make_async_copy(refs[i], refs[9 + i], refs[18].at[i]) for i in range(9)]
    for c in copies:
        c.start()
    for c in copies:
        c.wait()


def local(*args):
    shapes = (
        ((ROLES, 128, COLS), F32),
        ((ROLES, 128, COLS), F32),
        ((ROLES, 2 * FS, 64, COLS), BF16),
        ((ROLES, RANK, COLS), F32),
        ((ROLES, RANK, COLS), F32),
        ((HEADS, DIM), F32),
        ((HEADS, DIM), BF16),
        ((HEADS, DIM), F32),
        ((HEADS, DIM), F32),
    )
    vmem, dma = pltpu.VMEM, pltpu.SemaphoreType.DMA
    gates = vmem((HEADS, DIM), F32)
    moments = vmem((ROLES, RANK, COLS), F32)
    outs = pl.pallas_call(
        kernel,
        out_shape=[vmem(s, d) for s, d in shapes],
        in_specs=[pl.BlockSpec(memory_space=pl.ANY)] * 11,
        out_specs=[pl.BlockSpec(memory_space=vmem)] * 9,
        scratch_shapes=[
            vmem((BLOCKS, TOK, BLOCK), BF16),
            vmem((ROLES, TOK, COLS), BF16),
            vmem((HEADS, TOK), F32),
            vmem((HEADS, TOK), F32),
            vmem((ROLES, 128, COLS), F32),
            vmem((ROLES, 2 * FS, 2, 32, RANK), BF16),
            moments, moments, gates, gates, gates,
            vmem((2, COLS + HEADS, TOK), BF16),
            vmem((ROLES, 2 * COLS, DIM), BF16),
            vmem((HEADS, TOK), F32),
            vmem((HEADS, TOK), F32),
            vmem((FS, 8, 128), F32),
            moments,
            vmem((ROLES, 2, 3, 32, COLS), F32),
            vmem((ROLES, 2, 32, COLS), F32),
            vmem((ROLES, 2, 3, 8, COLS), F32),
            moments,
            vmem((FS, 2, 8, 128), F32),
            vmem((FS, 8, 128), F32),
            vmem((FS, 2, 8, 128), F32),
            vmem((ROLES, 128, COLS), F32),
            vmem((TP, 1, 128), F32),
            vmem((FS, 1, 128), F32),
            vmem((ROLES, 2 * FS, EARLY, COLS), F32),
            vmem((ROLES, RANK, 2 * COLS), BF16),
            dma((12,)), dma((BLOCKS,)), dma((ROLES,)),
            dma((4,)), dma((4,)), dma((ROLES,)), dma((ROLES, 4)), dma((2,)),
            dma((ROLES,)), dma((ROLES, 3)), dma((ROLES + 1,)), dma((ROLES + 1,)), dma((ROLES,)), dma((ROLES, 8)),
            dma((1,)), dma((8,)),
        ],
        compiler_params=pltpu.CompilerParams(
            collective_id=0, has_side_effects=True, vmem_limit_bytes=57 * 1024 * 1024
        ),
    )(*args)
    outs = pl.pallas_call(
        written,
        out_shape=[jax.ShapeDtypeStruct(s, d) for s, d in shapes],
        in_specs=[pl.BlockSpec(memory_space=vmem)] * 9,
        out_specs=[pl.BlockSpec(memory_space=pl.ANY)] * 9,
        scratch_shapes=[dma((9,))],
        compiler_params=pltpu.CompilerParams(vmem_limit_bytes=1024 * 1024),
    )(*(pltpu.with_memory_space_constraint(o, pltpu.VMEM) for o in outs))
    outs = list(outs)
    outs[2] = outs[2].reshape(ROLES, DIM, COLS)
    return tuple(outs)


def solution(mesh):
    placed = (
        P("fs", None),
        P(None, "fs", "tp"),
        P(None, "fs"),
        P(None, "fs"),
        P(None, "fs", "tp"),
        P(None, "fs", None),
        P(None, None, "tp"),
        P(None, None, "tp"),
        P(),
        P(),
        P(),
    )
    return jax.shard_map(
        local,
        mesh=mesh,
        in_specs=placed,
        out_specs=(
            P(None, "fs", "tp"),
            P(None, "fs", "tp"),
            P(None, None, "tp"),
            P(None, None, "tp"),
            P(None, None, "tp"),
            P(),
            P(),
            P(),
            P(),
        ),
        check_vma=False,
    )
```

```python
import functools

import jax
import jax.numpy as jnp
from jax import lax
from jax.experimental import pallas as pl
from jax.experimental.pallas import tpu as pltpu
from jax.sharding import PartitionSpec as P

BETA_ONE = 0.8
BETA_TWO = 0.9
LEARN = 0.001
MESH = pl.DeviceIdType.MESH
F32, BF16 = jnp.float32, jnp.bfloat16

FS, TP, RING = 16, 8, 4
ROLES, TOK, DIM, COLS, RANK, HEADS = 3, 3072, 2048, 256, 256, 16
BLOCK = 512
BLOCKS = DIM // BLOCK
EARLY = 16
TURN = TOK // BLOCKS


def minus_expm1(x):
    series = jnp.ones_like(x)
    for n in range(9, 1, -1):
        series = 1.0 + x * (1.0 / n) * series
    return jnp.where(jnp.abs(x) < 0.5, -x * series, 1.0 - jnp.exp(x))


def halves(x):
    upper = x.astype(BF16)
    return upper, (x - upper.astype(F32)).astype(BF16)


class Gather:
    def __init__(self, me, piece, many, send, recv, coarse=False):
        self.me, self.piece, self.many, self.send, self.recv, self.coarse = me, piece, many, send, recv, coarse
        x, z = me % RING, me // RING
        self.at = ((x, z), (z, x))

    def name(self, half, first, second):
        return second * RING + first if half == 0 else first * RING + second

    def sem(self, index):
        if index < 3:
            return self.recv.at[1 if self.coarse else 1 + index]
        e, kind = divmod(index - 3, 3)
        if kind == (0 if e < 2 else 1):
            return self.recv.at[(1 if e == 0 else 2) if self.coarse else 4 + e]
        return self.recv.at[0]

    def copy(self, half, index):
        p, q = self.at[half]
        turn = lambda a, b: (a + b + RING) % RING
        if index < 3:
            d = index + 1
            out, to = (p, q), (turn(p, d), q)
        else:
            e, kind = divmod(index - 3, 3)
            first = turn(p, -e)
            if kind == 0:
                out, to = (first, q), (p, turn(q, 1))
            elif kind == 1:
                out, to = (first, q), (p, turn(q, -1))
            elif e < 2:
                out, to = (first, turn(q, -1)), (p, turn(q, 1))
            else:
                out, to = (first, turn(q, 1)), (p, turn(q, -1))
        ref = self.piece(self.name(half, *out), half)
        return pltpu.make_async_remote_copy(
            ref, ref, self.send, self.sem(index), device_id={"fs": self.name(half, *to)}, device_id_type=MESH
        )

    def start(self, index):
        for half in (0, 1):
            self.copy(half, index).start()

    def arrived(self, index):
        self.whole(2, self.sem(index)).wait_recv()

    def first(self):
        for index in (1, 0, 2, 3, 4):
            self.start(index)

    def second(self, own=True, behind=(1, 3, 2)):
        if self.coarse:
            self.whole(8, self.recv.at[1]).wait_recv()
        if own:
            if not self.coarse:
                self.arrived(3)
            self.start(5)
        for e in behind:
            if not self.coarse:
                self.arrived(e - 1)
            self.start(3 + 3 * e)
            self.start(4 + 3 * e)

    def third(self):
        if self.coarse:
            self.whole(6, self.recv.at[2]).wait_recv()
        for e in (1, 3, 2):
            if not self.coarse:
                self.arrived(3 + 3 * e if e < 2 else 4 + 3 * e)
            self.start(5 + 3 * e)

    def whole(self, n, sem):
        ref = self.many(n)
        return pltpu.make_async_remote_copy(
            ref, ref, self.send, sem, device_id={"fs": (self.me + 1) % FS}, device_id_type=MESH
        )

    def last(self):
        self.whole(16, self.recv.at[0]).wait_recv()

    def drain(self):
        self.whole(30, self.recv.at[0]).wait_send()


def kernel(
    x_hbm, cot_hbm, logs_hbm, ccot_hbm, master_hbm, factors_hbm, first_hbm, second_hbm, gm_hbm, gf_hbm, gs_hbm,
    step_ref, new_ref, copy_ref, first_ref, second_ref, gnew_ref, gcopy_ref, gfirst_ref, gsecond_ref,
    x_v, cot_v, logs_v, ccot_v, master_v, fac_v, fm_v, sm_v, gm_v, gf_v, gs_v,
    lhs_v, grad_v, later_v, gate_v, gx_v, lowp_v, sum_a, sum_b, sum_c, low_v, gp_v, grs_v, gfull_v, prod_v, ss_v, st_v, early_v, dir_v,
    in_sem, x_sem, cot_sem, p_send, p_recv, s_send, s_recv, ss_sem, f_send, f_recv, d_send, d_recv, c_send, c_recv, e_send, e_recv,
):
    me, tp = lax.axis_index("fs"), lax.axis_index("tp")
    core = tp % 2

    barrier = pltpu.get_barrier_semaphore()

    @pl.loop(1, FS)
    def _(d):
        pl.semaphore_signal(barrier, inc=1, device_id={"fs": (me + d) % FS}, device_id_type=MESH)

    @pl.loop(1, TP)
    def _(d):
        pl.semaphore_signal(barrier, inc=1, device_id={"tp": (tp + d) % TP}, device_id_type=MESH)

    def load(src, dst, sem):
        return pltpu.make_async_copy(src, dst, sem)

    fac_in = [
        load(factors_hbm.at[:, pl.ds(pl.multiple_of(64 * h + 32 * core, 32), 32), :], fac_v.at[:, 2 * me + h, core], in_sem.at[h])
        for h in (0, 1)
    ]
    logs_in = load(logs_hbm, logs_v, in_sem.at[2])
    ccot_in = load(ccot_hbm, ccot_v, in_sem.at[3])
    cot_in = [load(cot_hbm.at[r], cot_v.at[r], cot_sem.at[r]) for r in range(ROLES)]
    x_in = [load(x_hbm.at[:, pl.ds(BLOCK * n, BLOCK)], x_v.at[n], x_sem.at[n]) for n in range(BLOCKS)]
    rest_in = [
        load(s, d, in_sem.at[4 + i])
        for i, (s, d) in enumerate(
            ((first_hbm, fm_v), (second_hbm, sm_v), (master_hbm, master_v), (gm_hbm, gm_v), (gf_hbm, gf_v), (gs_hbm, gs_v))
        )
    ]
    early_in = [load(master_hbm.at[:, pl.ds(64 * h, EARLY), :], early_v.at[:, 2 * me + h], in_sem.at[10 + h]) for h in (0, 1)]
    for c in (*fac_in, ccot_in, logs_in, cot_in[0], x_in[0], cot_in[1], *x_in[1:], cot_in[2], *early_in, *rest_in):
        c.start()

    def put(src, dst, send, recv, to):
        return pltpu.make_async_remote_copy(src, dst, send, recv, device_id=to, device_id_type=MESH)

    def to_peers(src, dst, k):
        @pl.loop(1, FS)
        def _(d):
            peer = (me + d) % FS
            put(src(peer), dst, p_send.at[k], p_recv.at[k], {"fs": peer}).start()

    def from_peers(ref, k):
        ref = ref.at[pl.ds(0, FS - 1)]
        put(ref, ref, p_send.at[k], p_recv.at[k], {"fs": (me + 1) % FS}).wait_recv()

    def sent(ref, k):
        ref = ref.at[pl.ds(0, FS - 1)]
        put(ref, ref, p_send.at[k], p_recv.at[k], {"fs": (me + 1) % FS}).wait_send()

    me_x, me_z = me % RING, me // RING
    at = ((me_x, me_z), (me_z, me_x))

    def device(half, first, second):
        return {"fs": second * RING + first if half == 0 else first * RING + second}

    def turn(a, d):
        return (a + d) % RING

    def rows(start, size):
        return pl.ds(pl.multiple_of(start, 8), size)

    def swap(r, phase):
        for half in (0, 1):
            p, q = at[half]
            for d in (1, 3, 2):
                if phase == 0:
                    to = (turn(p, d), q)
                    src = lowp_v.at[r, rows(128 * half + 32 * to[0], 32)]
                    dst = sum_a.at[r, half, d - 1]
                elif phase == 1:
                    to = (p, turn(q, d))
                    src = sum_b.at[r, half, rows(8 * to[1], 8)]
                    dst = sum_c.at[r, half, d - 1]
                elif phase == 2:
                    to = (p, turn(q, d))
                    src = dst = low_v.at[r, rows(128 * half + 32 * p + 8 * q, 8)]
                else:
                    to = (turn(p, d), q)
                    src = dst = low_v.at[r, rows(128 * half + 32 * p, 32)]
                put(src, dst, s_send.at[r], s_recv.at[r, phase], device(half, *to)).start()

    def whole(r, phase):
        ref = (sum_a.at[r], sum_c.at[r], low_v.at[r, pl.ds(0, 48)], low_v.at[r, pl.ds(0, 192)])[phase]
        return put(ref, ref, s_send.at[r], s_recv.at[r, phase], {"fs": (me + 1) % FS})

    def second_sum(r):
        whole(r, 0).wait_recv()
        for half in (0, 1):
            p, q = at[half]
            got = sum_a[r, half]
            sum_b[r, half] = lowp_v[r, rows(128 * half + 32 * p, 32)] + got[0] + got[1] + got[2]
        swap(r, 1)

    def first_spread(r):
        whole(r, 1).wait_recv()
        for half in (0, 1):
            p, q = at[half]
            got = sum_c[r, half]
            low_v[r, rows(128 * half + 32 * p + 8 * q, 8)] = sum_b[r, half, rows(8 * q, 8)] + got[0] + got[1] + got[2]
        swap(r, 2)

    def second_spread(r):
        whole(r, 2).wait_recv()
        swap(r, 3)

    facs = [
        Gather(
            me,
            lambda i, h, r=r: fac_v.at[r, 2 * i + h, core],
            lambda n, r=r: fac_v.at[r, pl.ds(0, n), core],
            f_send.at[r],
            f_recv.at[r],
            True,
        )
        for r in range(ROLES)
    ]
    fac_in[0].wait()
    fac_in[1].wait()
    pl.semaphore_wait(barrier, FS + TP - 2)
    facs[0].first()

    ccot_in.wait()
    logs_in.wait()
    small = lax.broadcasted_iota(jnp.int32, (8, 128), 1)
    sums = jnp.sum(ccot_v[...], axis=1, keepdims=True)
    ends = logs_v[:, TOK - 128 :][:, 127:128]
    message = jnp.where(small < 32, sums[:8], sums[8:])
    message = jnp.where(small < 64, message, ends[:8])
    gx_v[me] = jnp.where(small < 96, message, ends[8:])
    to_peers(lambda peer: gx_v.at[me], gx_v.at[me], 0)
    for r in range(1, ROLES):
        facs[r].first()

    lane = lax.broadcasted_iota(jnp.int32, (HEADS, TOK), 1)
    later = ccot_v[...]
    by = 1
    while by < TOK:
        later = later + jnp.where(lane < TOK - by, pltpu.roll(later, TOK - by, 1), 0.0)
        by *= 2
    later_v[...] = later
    logs = logs_v[...]
    gate_v[...] = minus_expm1(logs - pltpu.roll(logs, 1, 1))

    def across(r, side):
        return pltpu.make_async_remote_copy(
            fac_v.at[r, :, side], fac_v.at[r, :, side], d_send.at[r], d_recv.at[r],
            device_id={"tp": tp + 1 - 2 * core}, device_id_type=MESH,
        )

    early = Gather(
        me, lambda i, h: early_v.at[:, 2 * i + h], lambda n: early_v.at[:, pl.ds(0, n)], e_send.at[0], e_recv
    )

    def early_first():
        for c in early_in:
            c.wait()
        early.first()

    def other_gates(side):
        ref = gfull_v.at[:, side]
        return put(ref, ref, d_send.at[ROLES], d_recv.at[ROLES], {"tp": tp + 1 - 2 * core})

    def turned(r, n):
        span = pl.ds(pl.multiple_of(TURN * n, TURN), TURN)
        lhs_v[r % 2, 0:COLS, span] = cot_v[r, span, :].T

    def contract(r):
        fac = fac_v[r].reshape(DIM, RANK)
        both = jnp.dot(grad_v[r], fac, preferred_element_type=F32)
        lowp_v[r] = (both[:COLS] + both[COLS:]).T
        swap(r, 0)

    def finish(r):
        low = low_v[r]
        first = BETA_ONE * fm_v[r] + (1.0 - BETA_ONE) * low
        second = BETA_TWO * sm_v[r] + (1.0 - BETA_TWO) * low * low
        first_ref[r] = first
        second_ref[r] = second
        direction = first * lax.rsqrt(second)
        own = fac_v[r, pl.ds(2 * me, 2)].reshape(128, RANK)
        dir_v[r] = jnp.concatenate(halves(direction), axis=1)
        both = jnp.dot(own, dir_v[r], preferred_element_type=F32)
        prod_v[r] = both[:, :COLS] + both[:, COLS:]

    def early_rows(r, scale):
        fac = fac_v[r, :, 0, 0:EARLY, :].reshape(2 * FS * EARLY, RANK)
        both = jnp.dot(fac, dir_v[r], preferred_element_type=F32)
        prod = (both[:, :COLS] + both[:, COLS:]).reshape(2 * FS, EARLY, COLS)
        copy_ref[r, :, 0:EARLY, :] = (early_v[r] - LEARN * (scale * prod)).astype(BF16)

    cot_in[0].wait()

    @pl.loop(0, BLOCKS)
    def _(n):
        turned(0, n)

    def handed(r):
        facs[r].last()
        across(r, core).start()

    def joined(r):
        across(r, 1 - core).wait_recv()
        contract(r)

    events = ((1, facs[0].second), (2, facs[1].second), (3, facs[2].second),), ((0, facs[0].third), (1, facs[1].third), (2, facs[2].third), (3, functools.partial(handed, 0)), (3, early_first),), ((0, functools.partial(handed, 1)), (1, functools.partial(handed, 2)), (1, functools.partial(joined, 0)), (2, functools.partial(joined, 1)), (3, functools.partial(joined, 2)),)

    for r in range(ROLES):
        height = COLS + HEADS if r == 1 else COLS

        @pl.loop(0, BLOCKS)
        def _(n):
            if r == 0:
                load(x_hbm.at[:, pl.ds(pl.multiple_of(BLOCK * n, BLOCK), BLOCK)], x_v.at[n], x_sem.at[n]).wait()
            if r + 1 < ROLES:
                pl.when(n == 0)(cot_in[r + 1].wait)
                turned(r + 1, n)
            grad = jnp.dot(lhs_v[r % 2, 0:height, :], x_v[n], preferred_element_type=F32)
            upper, lower = halves(grad[:COLS])
            span = pl.ds(pl.multiple_of(BLOCK * n, BLOCK), BLOCK)
            grad_v[r, 0:COLS, span] = upper
            grad_v[r, COLS:, span] = lower
            if r == 1:
                for i in range(BLOCK // 128):
                    for c in (0, 1):
                        gp_v[(BLOCK // 128) * n + i, c] = grad[COLS + 8 * c : COLS + 8 * c + 8, 128 * i : 128 * i + 128]
            for event, work in events[r]:
                pl.when(n == event)(work)

        if r == 0:
            from_peers(gx_v, 0)
            carried = jnp.zeros((8, 128), F32)
            edge = jnp.zeros((8, 128), F32)
            for i in range(FS):
                message = gx_v[i]
                carried = carried + jnp.where(i > me, message, 0.0)
                edge = edge + jnp.where(i == me - 1, message, 0.0)
            carried = jnp.concatenate([carried[:, 0:1], carried[:, 32:33]], axis=0)
            edge = jnp.concatenate([edge[:, 64:65], edge[:, 96:97]], axis=0)
            lhs_v[1, COLS:, :] = ((later_v[...] + carried) * gate_v[...]).astype(BF16)
            start = logs_v[:, 0:128]
            start = start - jnp.where(lane[:, 0:128] == 0, edge, pltpu.roll(start, 1, 1))
            lhs_v[1, COLS:, 0:128] = ((later_v[:, 0:128] + carried) * minus_expm1(start)).astype(BF16)
        if r == 1:
            to_peers(lambda peer: gp_v.at[peer, core], grs_v.at[me], 1)
            grs_v[me] = gp_v[me, core]

    for c in rest_in:
        c.wait()

    def slice_squares(r):
        squares = jnp.zeros((8, COLS), F32)
        for half in (0, 1):
            p, q = at[half]
            own = rows(128 * half + 32 * p + 8 * q, 8)
            low = low_v[r, own]
            first = BETA_ONE * fm_v[r, own] + (1.0 - BETA_ONE) * low
            second = BETA_TWO * sm_v[r, own] + (1.0 - BETA_TWO) * low * low
            direction = first * lax.rsqrt(second)
            squares = squares + direction * direction
        return jnp.sum(squares[:, :128] + squares[:, 128:], axis=0, keepdims=True)

    from_peers(grs_v, 1)
    gfull_v[me, core] = jnp.sum(grs_v[...], axis=0)
    second_sum(0)
    second_sum(1)
    second_sum(2)
    first_spread(0)
    first_spread(1)
    early.second(True, (1, 3))
    first_spread(2)

    ss_v[tp] = slice_squares(0) + slice_squares(1) + slice_squares(2)

    @pl.loop(1, TP)
    def _(d):
        put(ss_v.at[tp], ss_v.at[tp], ss_sem.at[0], ss_sem.at[1], {"tp": (tp + d) % TP}).start()

    squares = put(ss_v.at[pl.ds(0, TP - 1)], ss_v.at[pl.ds(0, TP - 1)], ss_sem.at[0], ss_sem.at[1], {"tp": (tp + 1) % TP})
    second_spread(0)
    second_spread(1)
    early.second(False, (2,))
    squares.wait_recv()
    st_v[me] = jnp.sum(ss_v[...], axis=0)
    to_peers(lambda peer: st_v.at[me], st_v.at[me], 3)
    second_spread(2)
    to_peers(lambda peer: gfull_v.at[me, core], gfull_v.at[me, core], 2)
    whole(0, 3).wait_recv()
    finish(0)
    whole(1, 3).wait_recv()
    finish(1)
    early.third()
    whole(2, 3).wait_recv()
    finish(2)

    from_peers(st_v, 3)
    total = jnp.sum(jnp.sum(st_v[...], axis=0), keepdims=True)
    scale = lax.rsqrt(total * (1.0 / (ROLES * RANK * COLS * TP)) + 1e-06)
    copies = [
        Gather(
            me,
            lambda i, h, r=r: copy_ref.at[r, 2 * i + h, pl.ds(EARLY, 64 - EARLY)],
            lambda n, r=r: copy_ref.at[r, pl.ds(0, n), pl.ds(EARLY, 64 - EARLY)],
            c_send.at[r],
            c_recv.at[r],
        )
        for r in range(ROLES)
    ]
    for r in range(ROLES):
        step = scale * prod_v[r]
        new = master_v[r] - LEARN * step
        step_ref[r] = step
        new_ref[r] = new
        copy_ref[r, pl.ds(2 * me, 2), EARLY:, :] = new.astype(BF16).reshape(2, 64, COLS)[:, EARLY:, :]
        copies[r].first()

    from_peers(grs_v, 2)
    other_gates(core).start()
    other_gates(1 - core).wait_recv()
    for i in range(FS):
        cut = slice(128 * i, 128 * i + 128)
        gate = gfull_v[i].reshape(HEADS, 128)
        first = BETA_ONE * gf_v[:, cut] + (1.0 - BETA_ONE) * gate
        second = BETA_TWO * gs_v[:, cut] + (1.0 - BETA_TWO) * gate * gate
        new = gm_v[:, cut] - LEARN * (first * lax.rsqrt(second))
        gfirst_ref[:, cut] = first
        gsecond_ref[:, cut] = second
        gnew_ref[:, cut] = new
        gcopy_ref[:, cut] = new.astype(BF16)
    squares.wait_send()
    for r in range(ROLES):
        across(r, core).wait_send()
        put(lowp_v.at[pl.ds(0, 2), pl.ds(0, 240)], lowp_v.at[pl.ds(0, 2), pl.ds(0, 240)], s_send.at[r], s_recv.at[r, 0], {"fs": (me + 1) % FS}).wait_send()
    sent(gx_v, 0)
    sent(grs_v, 1)
    sent(grs_v, 2)
    other_gates(core).wait_send()
    sent(st_v, 3)
    for r in range(ROLES):
        facs[r].drain()

    early.last()
    for r in range(ROLES):
        early_rows(r, scale)
    early.drain()

    for step in ("second", "third", "last", "drain"):
        for gather in copies:
            getattr(gather, step)()


def written(*refs):
    copies = [pltpu.make_async_copy(refs[i], refs[9 + i], refs[18].at[i]) for i in range(9)]
    for c in copies:
        c.start()
    for c in copies:
        c.wait()


def local(*args):
    shapes = (
        ((ROLES, 128, COLS), F32),
        ((ROLES, 128, COLS), F32),
        ((ROLES, 2 * FS, 64, COLS), BF16),
        ((ROLES, RANK, COLS), F32),
        ((ROLES, RANK, COLS), F32),
        ((HEADS, DIM), F32),
        ((HEADS, DIM), BF16),
        ((HEADS, DIM), F32),
        ((HEADS, DIM), F32),
    )
    vmem, dma = pltpu.VMEM, pltpu.SemaphoreType.DMA
    gates = vmem((HEADS, DIM), F32)
    moments = vmem((ROLES, RANK, COLS), F32)
    outs = pl.pallas_call(
        kernel,
        out_shape=[vmem(s, d) for s, d in shapes],
        in_specs=[pl.BlockSpec(memory_space=pl.ANY)] * 11,
        out_specs=[pl.BlockSpec(memory_space=vmem)] * 9,
        scratch_shapes=[
            vmem((BLOCKS, TOK, BLOCK), BF16),
            vmem((ROLES, TOK, COLS), BF16),
            vmem((HEADS, TOK), F32),
            vmem((HEADS, TOK), F32),
            vmem((ROLES, 128, COLS), F32),
            vmem((ROLES, 2 * FS, 2, 32, RANK), BF16),
            moments, moments, gates, gates, gates,
            vmem((2, COLS + HEADS, TOK), BF16),
            vmem((ROLES, 2 * COLS, DIM), BF16),
            vmem((HEADS, TOK), F32),
            vmem((HEADS, TOK), F32),
            vmem((FS, 8, 128), F32),
            moments,
            vmem((ROLES, 2, 3, 32, COLS), F32),
            vmem((ROLES, 2, 32, COLS), F32),
            vmem((ROLES, 2, 3, 8, COLS), F32),
            moments,
            vmem((FS, 2, 8, 128), F32),
            vmem((FS, 8, 128), F32),
            vmem((FS, 2, 8, 128), F32),
            vmem((ROLES, 128, COLS), F32),
            vmem((TP, 1, 128), F32),
            vmem((FS, 1, 128), F32),
            vmem((ROLES, 2 * FS, EARLY, COLS), F32),
            vmem((ROLES, RANK, 2 * COLS), BF16),
            dma((12,)), dma((BLOCKS,)), dma((ROLES,)),
            dma((4,)), dma((4,)), dma((ROLES,)), dma((ROLES, 4)), dma((2,)),
            dma((ROLES,)), dma((ROLES, 3)), dma((ROLES + 1,)), dma((ROLES + 1,)), dma((ROLES,)), dma((ROLES, 8)),
            dma((1,)), dma((8,)),
        ],
        compiler_params=pltpu.CompilerParams(
            collective_id=0, has_side_effects=True, vmem_limit_bytes=57 * 1024 * 1024
        ),
    )(*args)
    outs = pl.pallas_call(
        written,
        out_shape=[jax.ShapeDtypeStruct(s, d) for s, d in shapes],
        in_specs=[pl.BlockSpec(memory_space=vmem)] * 9,
        out_specs=[pl.BlockSpec(memory_space=pl.ANY)] * 9,
        scratch_shapes=[dma((9,))],
        compiler_params=pltpu.CompilerParams(vmem_limit_bytes=1024 * 1024),
    )(*(pltpu.with_memory_space_constraint(o, pltpu.VMEM) for o in outs))
    outs = list(outs)
    outs[2] = outs[2].reshape(ROLES, DIM, COLS)
    return tuple(outs)


def solution(mesh):
    placed = (
        P("fs", None),
        P(None, "fs", "tp"),
        P(None, "fs"),
        P(None, "fs"),
        P(None, "fs", "tp"),
        P(None, "fs", None),
        P(None, None, "tp"),
        P(None, None, "tp"),
        P(),
        P(),
        P(),
    )
    return jax.shard_map(
        local,
        mesh=mesh,
        in_specs=placed,
        out_specs=(
            P(None, "fs", "tp"),
            P(None, "fs", "tp"),
            P(None, None, "tp"),
            P(None, None, "tp"),
            P(None, None, "tp"),
            P(),
            P(),
            P(),
            P(),
        ),
        check_vma=False,
    )
```
